512 devices in a mesh: grp: 2 (over y), kv: 16 (over z), tp: 16 (over x, core).
Axes of the slice: x: 8, y: 2, z: 16, core: 2. Of those that a mesh axis runs over, the one named last changes fastest.
The devices are a block of a 8x16x16 slice.
Arguments:
- tokens: bfloat16 [256, 4096], P('grp', 'kv'), parts along dimension 0, may hold values from -36 to 36
- span_lengths: int32 [256], P(('grp', 'kv')), parts along dimension 0, may hold values from 1 to 256, 13107 in all
- block_state: float32 [256, 64, 32, 64], P(('grp', 'kv'), 'tp'), parts along dimension 0, may hold values from -96 to 96
- key_cache: bfloat16 [256, 2048, 256], P(('grp', 'kv'), 'tp'), parts along dimension 0, may hold values from -6 to 6
- value_cache: bfloat16 [256, 4096, 256], P(('grp', 'kv'), 'tp'), parts along dimension 0, may hold values from -6 to 6
- decay_cache: float32 [256, 2048, 256], P(('grp', 'kv'), 'tp'), parts along dimension 0, may hold values from -34 to 0, as said below
- attn_gain: float32 [4096], P('kv'), may hold values from 0.1 to 1.9
- query_weight: bfloat16 [4096, 2048], P('kv', 'tp'), may hold values from -0.09375 to 0.09375
- key_weight: bfloat16 [4096, 2048], P('kv', 'tp'), may hold values from -0.09375 to 0.09375
- value_weight: bfloat16 [4096, 4096], P('kv', 'tp'), may hold values from -0.09375 to 0.09375
- gate_weight: bfloat16 [4096, 4096], P('kv', 'tp'), may hold values from -0.09375 to 0.09375
- decay_matrix: bfloat16 [4096, 2048], P('kv', 'tp'), may hold values from -0.09375 to 0.09375
- decay_offset_bias: float32 [2048], P('tp'), may hold values from -1.4 to 6
- head_gain: float32 [64], replicated, may hold values from 0.1 to 1.9
- out_weight: bfloat16 [4096, 4096], P('tp', 'kv'), may hold values from -0.09375 to 0.09375
- mixer_gain: float32 [4096], P('kv'), may hold values from 0.1 to 1.9
- up_weight: bfloat16 [4096, 16384], P('kv', 'tp'), may hold values from -0.09375 to 0.09375
- down_weight: bfloat16 [16384, 4096], P('tp', 'kv'), may hold values from -0.046875 to 0.046875
Outputs:
- layer_out: bfloat16 [256, 4096], P('grp', 'kv'), parts along dimension 0
The draws below stay inside these ranges and needn't reach their ends.
There are 2 independent parts, one for each index of `grp`. The reference program is written for one: setup_inputs(seed, part) draws one part's arguments, and reference() takes and returns one part's arrays. A program takes and returns all parts, laid end to end along the dimension named above; an argument that names none is the same for every part. Nothing has to cross between parts.
Inputs may be any that keep to these rules, and one draw needn't show every extreme that they name: Cached positions at index span_lengths - 1 and beyond are unused. `decay_cache`: Non-increasing along positions.
All inputs are finite; a program needn't handle non-finite values. No bound on the sum of `span_lengths` on one device may be relied on, other than what follows from the above.
Results may differ from the reference program's by a relative error of at most 0.005.
The reference program's roundings to bfloat16 on the way count: a program that leaves them out, or rounds other values in their place, can miss the bound.
Values may be sent and summed in bfloat16 or wider, within the bound.
No kernel may reach another device: no remote copies, remote signals or barrier semaphores. Data moves between devices by JAX's collectives and lax.ppermute only.
A program may use at most 64 MiB of HBM per device.

```python
import math
import jax
import jax.numpy as jnp
import numpy as np
from jax import lax

D = 4096
HEAD_NUMBER = 64
KEY_WIDTH = 32
DV = 64
FF = 16384
SEQUENCE_NUMBER = 128
OPEN_POSITIONS = 256


def draw_tokens(key, part):
    key_base, key_rows = jax.random.split(jax.random.fold_in(key, 11))
    column = jnp.arange(D, dtype=jnp.float32) / (D - 1)
    base = jax.random.truncated_normal(key_base, -4.0, 4.0, (SEQUENCE_NUMBER, D), jnp.float32)
    column_scale = jnp.exp(math.log(0.3) + column * math.log(10.0))
    scale_per_row = jnp.exp(jax.random.uniform(key_rows, (SEQUENCE_NUMBER, 1), jnp.float32, math.log(0.3), math.log(3.0)))
    return (base * column_scale * scale_per_row).astype(jnp.bfloat16)


def draw_decay_offset_bias(key, part):
    key_head, key_fast, key_slow = jax.random.split(jax.random.fold_in(key, 23), 3)
    fast_share = 0.5
    fast_head = jax.random.uniform(key_head, (HEAD_NUMBER,), jnp.float32) < fast_share
    fast_channel = jnp.repeat(fast_head, KEY_WIDTH)
    fast_value = jax.random.uniform(key_fast, (HEAD_NUMBER * KEY_WIDTH,), jnp.float32, -1.4, 0.4)
    slow_value = jax.random.uniform(key_slow, (HEAD_NUMBER * KEY_WIDTH,), jnp.float32, 3.0, 6.0)
    return jnp.where(fast_channel, fast_value, slow_value).astype(jnp.float32)


def draw_decay_cache(key, part):
    every_key_rows = jax.random.split(jax.random.fold_in(key, 37), 7)
    fast_share = 0.5
    fast_head = jax.random.uniform(every_key_rows[0], (SEQUENCE_NUMBER, HEAD_NUMBER), jnp.float32) < fast_share
    fast_channel = jnp.repeat(fast_head, KEY_WIDTH, axis=1)
    fast_rate = jnp.exp(jax.random.uniform(every_key_rows[1], (SEQUENCE_NUMBER, HEAD_NUMBER * KEY_WIDTH), jnp.float32, math.log(1.0 / 80.0), math.log(1.0 / 30.0)))
    slow_rate = jnp.exp(jax.random.uniform(every_key_rows[2], (SEQUENCE_NUMBER, HEAD_NUMBER * KEY_WIDTH), jnp.float32, math.log(0.1), math.log(0.5))) / OPEN_POSITIONS
    sequence_factor = jnp.exp(jax.random.uniform(every_key_rows[3], (SEQUENCE_NUMBER, 1), jnp.float32, math.log(0.5), math.log(2.0)))
    rate = jnp.where(fast_channel, fast_rate, slow_rate) * sequence_factor
    every_step_index = -rate[:, :, None] * jax.random.uniform(every_key_rows[4], (SEQUENCE_NUMBER, HEAD_NUMBER * KEY_WIDTH, OPEN_POSITIONS), jnp.float32, 0.5, 1.5)
    token_group_start = jax.random.randint(every_key_rows[5], (SEQUENCE_NUMBER, HEAD_NUMBER, 2), 0, OPEN_POSITIONS)
    token_group_length = jax.random.uniform(every_key_rows[6], (SEQUENCE_NUMBER, HEAD_NUMBER, 2), jnp.float32, math.log(0.6), math.log(0.8))
    token_place = jnp.arange(OPEN_POSITIONS, dtype=jnp.int32)
    token_group = jnp.sum(jnp.where(token_group_start[..., None] == token_place, token_group_length[..., None], 0.0), axis=2)
    token_group = jnp.repeat(token_group, KEY_WIDTH, axis=1)
    return jnp.cumsum(every_step_index + token_group, axis=-1).astype(jnp.float32)


def levels(rng, extent, pieces, smallest, high):
    factor_of = 1.0
    for dim, parts in pieces:
        heights = jax.random.uniform(jax.random.fold_in(jax.random.fold_in(rng, 6), dim), (parts,), jnp.float32, smallest / len(pieces), high / len(pieces))
        factor_of = factor_of * jnp.repeat(jnp.exp(heights), extent[dim] // parts).reshape((-1,) + (1,) * (len(extent) - 1 - dim))
    return factor_of


def length_profile(count, total, bound, skew):
    weights = [(1 << 20) // math.isqrt(rank ** skew) + 1 for rank in range(2, count + 1)]
    spare, given = total - bound - (count - 1), [1] * (count - 1)
    while spare > 0:
        candidates = [i for i in range(count - 1) if given[i] < bound]
        whole, budget = sum([weights[i] for i in candidates]), spare
        for i in candidates:
            extra = min(bound - given[i], max(1, budget * weights[i] // whole), spare)
            given[i] = given[i] + extra
            spare = spare - extra
    return np.array([bound] + given)


def uneven_parts(rng, number_of, total, bound, skew):
    if number_of == 2:
        one = jax.random.randint(rng, (), max(1, total - bound), min(bound, total - 1) + 1)
        return jnp.stack([one, total - one])
    tallies = jnp.asarray(length_profile(number_of, total, bound, skew), jnp.int32)
    couples = (number_of - 1) // 2
    donor, taker = tallies[1:1 + 2 * couples:2], tallies[2:2 + 2 * couples:2]
    room = jnp.minimum(donor - 1, bound - taker)
    moved = jax.random.randint(jax.random.fold_in(rng, 1), (couples,), 0, 1 << 20) % (room + 1)
    tallies = tallies.at[1:1 + 2 * couples:2].set(donor - moved).at[2:2 + 2 * couples:2].set(taker + moved)
    return tallies[jax.random.permutation(jax.random.fold_in(rng, 2), number_of)]


def noise(stream_key, dims, spread, reach, shards=(), kind=jnp.bfloat16):
    entries = spread * jax.random.normal(stream_key, dims, jnp.float32)
    if shards:
        entries = entries * levels(stream_key, dims, shards, -0.22, 0.18)
    return jnp.clip(entries, -reach, reach).astype(kind)


def setup_inputs(seed: int = 0, part: int = 0) -> dict:
    key_list = jax.random.split(jax.random.key(seed), 19)
    part_keys = jax.random.split(jax.random.fold_in(key_list[18], part), 19)
    return {
        "tokens": draw_tokens(jax.random.fold_in(jax.random.fold_in(key_list[18], part), 71), part),
        "span_lengths": uneven_parts(part_keys[1], SEQUENCE_NUMBER, SEQUENCE_NUMBER * OPEN_POSITIONS * 2 // 5, OPEN_POSITIONS, 2).astype(jnp.int32),
        "block_state": noise(part_keys[2], (SEQUENCE_NUMBER, HEAD_NUMBER, KEY_WIDTH, DV), 16.0, 96.0, ((0, 16), (1, 16)), jnp.float32),
        "key_cache": noise(part_keys[3], (SEQUENCE_NUMBER, HEAD_NUMBER * KEY_WIDTH, OPEN_POSITIONS), 1.0, 6.0, ((0, 16), (1, 16))),
        "value_cache": noise(part_keys[4], (SEQUENCE_NUMBER, HEAD_NUMBER * DV, OPEN_POSITIONS), 1.0, 6.0, ((0, 16), (1, 16))),
        "decay_cache": draw_decay_cache(jax.random.fold_in(jax.random.fold_in(key_list[18], part), 71), part),
        "attn_gain": jnp.clip(1.0 + 0.18 * jax.random.normal(key_list[6], (D,), jnp.float32), 0.1, 1.9),
        "query_weight": noise(key_list[7], (D, HEAD_NUMBER * KEY_WIDTH), D ** -0.5, 0.09375, ((0, 16), (1, 16))),
        "key_weight": noise(key_list[8], (D, HEAD_NUMBER * KEY_WIDTH), D ** -0.5, 0.09375, ((0, 16), (1, 16))),
        "value_weight": noise(key_list[9], (D, HEAD_NUMBER * DV), D ** -0.5, 0.09375, ((0, 16), (1, 16))),
        "gate_weight": noise(key_list[10], (D, HEAD_NUMBER * DV), D ** -0.5, 0.09375, ((0, 16), (1, 16))),
        "decay_matrix": noise(key_list[11], (D, HEAD_NUMBER * KEY_WIDTH), D ** -0.5, 0.09375, ((0, 16), (1, 16))),
        "decay_offset_bias": draw_decay_offset_bias(jax.random.fold_in(key_list[18], 71), part),
        "head_gain": jnp.clip(1.0 + 0.18 * jax.random.normal(key_list[13], (DV,), jnp.float32), 0.1, 1.9),
        "out_weight": noise(key_list[14], (HEAD_NUMBER * DV, D), (HEAD_NUMBER * DV) ** -0.5, 0.09375, ((0, 16), (1, 16))),
        "mixer_gain": jnp.clip(1.0 + 0.18 * jax.random.normal(key_list[15], (D,), jnp.float32), 0.1, 1.9),
        "up_weight": noise(key_list[16], (D, FF), D ** -0.5, 0.09375, ((0, 16), (1, 16))),
        "down_weight": noise(key_list[17], (FF, D), FF ** -0.5, 0.046875, ((0, 16), (1, 16))),
    }


NORM_EPS = 1e-06
DECAY_SOFTNESS = 16.0

def span_attend(inputs):
    query, logarithm_decay, keys_span, values_span, decays_span, start_state, length, key_new, value_new = inputs
    token_place = jnp.arange(OPEN_POSITIONS, dtype=jnp.int32)
    previous = lax.optimization_barrier(jnp.sum(jnp.where(token_place[None, None, :] == length - 2, decays_span, 0.0), axis=-1))
    now_decay = previous + logarithm_decay
    in_use = (token_place < length - 1)[None, None, :]
    factor = jnp.where(in_use, jnp.exp(now_decay[:, :, None] - decays_span), 0.0)
    scores = lax.optimization_barrier(jnp.sum(query[:, :, None] * keys_span.astype(jnp.float32) * factor, axis=1))
    rounded = lax.optimization_barrier(scores.astype(jnp.bfloat16)).astype(jnp.float32)
    history = jnp.einsum('hs,hvs->hv', rounded, values_span.astype(jnp.float32))
    carried = jnp.einsum('hc,hcv->hv', query * jnp.exp(now_decay), start_state, precision=lax.Precision.HIGHEST)
    own_term = lax.optimization_barrier(jnp.sum(query * key_new, axis=-1, keepdims=True)) * value_new
    return carried + history + own_term

def reference(tokens, span_lengths, block_state, key_cache, value_cache, decay_cache, attn_gain, query_weight, key_weight, value_weight, gate_weight, decay_matrix, decay_offset_bias, head_gain, out_weight, mixer_gain, up_weight, down_weight):
    whole_rows = tokens.astype(jnp.float32)
    mean_square = lax.optimization_barrier(jnp.mean(whole_rows * whole_rows, axis=1, keepdims=True))
    scale_per_row = lax.rsqrt(mean_square + NORM_EPS)
    scaled = (whole_rows * attn_gain).astype(jnp.bfloat16)

    def apply_projection(weight):
        return jnp.dot(scaled, weight, preferred_element_type=jnp.float32) * scale_per_row
    query = apply_projection(query_weight) * KEY_WIDTH ** (-0.5)
    key_new = apply_projection(key_weight)
    value_new = apply_projection(value_weight)
    gate = apply_projection(gate_weight)
    logarithm_decay = jax.nn.log_sigmoid(apply_projection(decay_matrix) + decay_offset_bias) / DECAY_SOFTNESS
    raw = lax.map(span_attend, (query.reshape(SEQUENCE_NUMBER, HEAD_NUMBER, KEY_WIDTH), logarithm_decay.reshape(SEQUENCE_NUMBER, HEAD_NUMBER, KEY_WIDTH), key_cache.reshape(SEQUENCE_NUMBER, HEAD_NUMBER, KEY_WIDTH, OPEN_POSITIONS), value_cache.reshape(SEQUENCE_NUMBER, HEAD_NUMBER, DV, OPEN_POSITIONS), decay_cache.reshape(SEQUENCE_NUMBER, HEAD_NUMBER, KEY_WIDTH, OPEN_POSITIONS), block_state, span_lengths.astype(jnp.int32), key_new.reshape(SEQUENCE_NUMBER, HEAD_NUMBER, KEY_WIDTH), value_new.reshape(SEQUENCE_NUMBER, HEAD_NUMBER, DV)))
    normed = raw * lax.rsqrt(lax.optimization_barrier(jnp.mean(raw * raw, axis=-1, keepdims=True)) + NORM_EPS) * head_gain
    mixed = (normed.reshape(SEQUENCE_NUMBER, HEAD_NUMBER * DV) * jax.nn.silu(gate)).astype(jnp.bfloat16)
    attn_out = jnp.dot(mixed, out_weight, preferred_element_type=jnp.float32)
    resid = (whole_rows + attn_out).astype(jnp.bfloat16)
    resid_rows = resid.astype(jnp.float32)
    mixer_square = lax.optimization_barrier(jnp.mean(resid_rows * resid_rows, axis=1, keepdims=True))
    mixer_scaled = (resid_rows * mixer_gain).astype(jnp.bfloat16)
    before = jnp.dot(mixer_scaled, up_weight, preferred_element_type=jnp.float32) * lax.rsqrt(mixer_square + NORM_EPS)
    hidden = jnp.square(jax.nn.relu(before)).astype(jnp.bfloat16)
    return (resid_rows + jnp.dot(hidden, down_weight, preferred_element_type=jnp.float32)).astype(jnp.bfloat16)
```

```python
import jax
import jax.numpy as jnp
from jax import lax
from jax.sharding import Mesh, PartitionSpec as P

D = 4096
KEY_WIDTH = 32
DV = 64
LANES = 128
CORES = 2

NORM_EPS = 1e-06
DECAY_SOFTNESS = 16.0


def exchange(pieces, axes):
    return lax.all_to_all(pieces, axes, 0, 0, tiled=True)


def to_everyone(value, axes):
    peers = lax.axis_size(axes)
    return exchange(jnp.broadcast_to(value[None], (peers, *value.shape)), axes)


def square_lanes(square):
    high = lax.reduce_precision(square, 8, 7)
    low = (square - high).astype(jnp.bfloat16)
    both = jnp.concatenate([high.astype(jnp.bfloat16), low], axis=1)
    return jnp.pad(both, [(0, 0), (0, LANES - both.shape[1])])


def dot(a, b):
    return jnp.dot(a, b, preferred_element_type=jnp.float32)


def shards(
    tokens,
    span_lengths,
    block_state,
    key_cache,
    value_cache,
    decay_cache,
    attn_gain,
    query_weight,
    key_weight,
    value_weight,
    gate_weight,
    decay_matrix,
    decay_offset_bias,
    head_gain,
    out_weight,
    mixer_gain,
    up_weight,
    down_weight,
):
    f32, bf16 = jnp.float32, jnp.bfloat16
    seq_count, head_count = block_state.shape[:2]
    span_size = key_cache.shape[2]
    peers = lax.axis_size("kv")
    core = lax.axis_index("core")
    half = seq_count // CORES
    rows_half = peers * half
    keys, values = head_count * KEY_WIDTH, head_count * DV

    whole_rows = tokens.astype(f32)
    square_sum = jnp.sum(whole_rows * whole_rows, axis=1, keepdims=True)
    scaled = (whole_rows * attn_gain).astype(bf16)
    parts = [
        dot(scaled, w).astype(bf16)
        for w in (query_weight, key_weight, decay_matrix, value_weight, gate_weight)
    ]
    sent = jnp.concatenate([*parts, square_lanes(square_sum)], axis=1)
    arrived = exchange(sent.reshape(peers, seq_count, -1), "kv")

    swap = [(c, CORES - 1 - c) for c in range(CORES)]
    out_other = lax.ppermute(out_weight, "core", swap)
    up_other = lax.ppermute(up_weight, "core", swap)
    down_other = lax.ppermute(down_weight, "core", swap)
    out_first = jnp.where(core == 0, out_weight, out_other)
    out_second = jnp.where(core == 0, out_other, out_weight)
    own_tokens = lax.dynamic_index_in_dim(
        tokens.reshape(peers, CORES, half, -1), core, 1, keepdims=False
    ).reshape(rows_half, -1)

    total = jnp.sum(arrived.astype(f32), axis=0)
    query_sum, key_sum, decay_sum, value_sum, gate_sum, squares = jnp.split(
        total, [keys, 2 * keys, 3 * keys, 3 * keys + values, 3 * keys + 2 * values], axis=1
    )
    scale_per_row = lax.rsqrt((squares[:, :1] + squares[:, 1:2]) / D + NORM_EPS)
    query = (query_sum * scale_per_row * KEY_WIDTH ** (-0.5)).reshape(
        seq_count, head_count, KEY_WIDTH
    )
    key_new = (key_sum * scale_per_row).reshape(seq_count, head_count, KEY_WIDTH)
    value_new = (value_sum * scale_per_row).reshape(seq_count, head_count, DV)
    gate = gate_sum * scale_per_row
    logarithm_decay = (
        jax.nn.log_sigmoid(decay_sum * scale_per_row + decay_offset_bias) / DECAY_SOFTNESS
    )
    token_place = lax.broadcasted_iota(jnp.int32, (1, 1, span_size), 2)
    lengths_now = span_lengths[:, None, None]
    previous = jnp.sum(jnp.where(token_place == lengths_now - 2, decay_cache, 0.0), axis=-1)
    now_decay = (previous + logarithm_decay).reshape(seq_count, head_count, KEY_WIDTH)
    decays_span = decay_cache.reshape(seq_count, head_count, KEY_WIDTH, span_size)
    in_use = (token_place < lengths_now - 1)[:, :, None, :]
    factor = jnp.where(in_use, jnp.exp(now_decay[..., None] - decays_span), 0.0)
    keys_span = key_cache.reshape(seq_count, head_count, KEY_WIDTH, span_size)
    scores = jnp.sum(query[..., None] * keys_span.astype(f32) * factor, axis=2)
    scores_low = scores.astype(bf16)
    values_span = value_cache.reshape(seq_count, head_count, DV, span_size)
    history = jnp.einsum("nhs,nhvs->nhv", scores_low, values_span, preferred_element_type=f32)
    carried = jnp.einsum(
        "nhc,nhcv->nhv", query * jnp.exp(now_decay), block_state, precision=lax.Precision.HIGHEST
    )
    own_term = jnp.sum(query * key_new, axis=-1, keepdims=True) * value_new
    raw = carried + history + own_term
    normed = raw * lax.rsqrt(jnp.mean(raw * raw, axis=-1, keepdims=True) + NORM_EPS) * head_gain
    mixed = (normed.reshape(seq_count, values) * jax.nn.silu(gate)).astype(bf16)

    spread = jnp.broadcast_to(
        mixed.reshape(1, CORES, half, values), (peers, CORES, half, values)
    ).reshape(peers * CORES, half, values)
    heads = exchange(spread, ("kv", "core")).reshape(peers, CORES, half, values)
    attn_terms = dot(heads[:, 0].reshape(rows_half, values), out_first) + dot(
        heads[:, 1].reshape(rows_half, values), out_second
    )
    attn_out = jnp.sum(to_everyone(attn_terms.astype(bf16), "x").astype(f32), axis=0)
    resid = (own_tokens.astype(f32) + attn_out).astype(bf16)
    resid_rows = resid.astype(f32)
    mixer_square = jnp.sum(resid_rows * resid_rows, axis=1, keepdims=True)
    mixer_scaled = (resid_rows * mixer_gain).astype(bf16)
    up_sent = jnp.concatenate(
        [
            dot(mixer_scaled, up_weight).astype(bf16),
            dot(mixer_scaled, up_other).astype(bf16),
            square_lanes(mixer_square),
        ],
        axis=1,
    )
    up_total = jnp.sum(exchange(up_sent.reshape(peers, half, -1), "kv").astype(f32), axis=0)
    hidden_count = up_weight.shape[1] * CORES
    before, squares = up_total[:, :hidden_count], up_total[:, hidden_count:]
    mixer_scale = lax.rsqrt((squares[:, :1] + squares[:, 1:2]) / D + NORM_EPS)
    hidden = jnp.square(jax.nn.relu(before * mixer_scale)).astype(bf16)
    every = to_everyone(hidden, "kv").reshape(rows_half, hidden_count)
    own_count = up_weight.shape[1]
    down_terms = dot(every[:, :own_count], down_weight) + dot(every[:, own_count:], down_other)
    mixer_out = jnp.sum(to_everyone(down_terms.astype(bf16), "x").astype(f32), axis=0)
    own_out = (resid_rows + mixer_out).astype(bf16)
    both = to_everyone(own_out, "core").reshape(CORES, peers, half, -1)
    return jnp.swapaxes(both, 0, 1).reshape(peers * seq_count, -1)


def solution(mesh):
    sizes = dict(mesh.shape)
    fine = Mesh(
        mesh.devices.reshape(sizes["grp"], sizes["kv"], sizes["tp"] // CORES, CORES),
        ("grp", "kv", "x", "core"),
    )
    tp = ("x", "core")
    placed = (
        P("grp", "kv"),
        P(("grp", "kv")),
        P(("grp", "kv"), tp, None, None),
        P(("grp", "kv"), tp, None),
        P(("grp", "kv"), tp, None),
        P(("grp", "kv"), tp, None),
        P("kv"),
        P("kv", tp),
        P("kv", tp),
        P("kv", tp),
        P("kv", tp),
        P("kv", tp),
        P(tp),
        P(),
        P(tp, "kv"),
        P("kv"),
        P("kv", tp),
        P(tp, "kv"),
    )
    return jax.shard_map(
        shards, mesh=fine, in_specs=placed, out_specs=P("grp", "kv"), check_vma=False
    )
```

```python
import jax
import jax.numpy as jnp
from jax import lax
from jax.experimental import pallas as pl
from jax.experimental.pallas import tpu as pltpu
from jax.sharding import Mesh, PartitionSpec as P

D = 4096
KEY_WIDTH = 32
DV = 64
LANES = 128
SUBLANES = 8
CORES = 2

NORM_EPS = 1e-06
DECAY_SOFTNESS = 16.0

f32, bf16 = jnp.float32, jnp.bfloat16


def exchange(pieces, axes):
    return lax.all_to_all(pieces, axes, 0, 0, tiled=True)


def to_everyone(value, axes):
    peers = lax.axis_size(axes)
    return exchange(jnp.broadcast_to(value[None], (peers, *value.shape)), axes)


def dot(a, b):
    return jnp.dot(a, b, preferred_element_type=f32)


def square_lanes(square):
    high = lax.reduce_precision(square, 8, 7)
    lane = lax.broadcasted_iota(jnp.int32, (square.shape[0], LANES), 1)
    return jnp.where(lane == 0, high, jnp.where(lane == 1, square - high, 0.0)).astype(bf16)


def project_kernel(tokens, gain, *refs):
    *weights, out = refs
    rows = tokens[...].astype(f32)
    square = jnp.sum(rows * rows, axis=1, keepdims=True)
    scaled = (rows * gain[...]).astype(bf16)
    start = 0
    for w in weights:
        width = w.shape[1]
        out[:, start : start + width] = dot(scaled, w[...]).astype(bf16)
        start += width
    high = square.astype(bf16).astype(f32)
    lane = lax.broadcasted_iota(jnp.int32, (rows.shape[0], LANES), 1)
    out[:, start:] = jnp.where(lane == 0, high, jnp.where(lane == 1, square - high, 0.0)).astype(
        bf16
    )


def project(tokens, gain, weights):
    width = sum(w.shape[1] for w in weights) + LANES
    return pl.pallas_call(
        project_kernel,
        out_shape=jax.ShapeDtypeStruct((tokens.shape[0], width), bf16),
        name="project",
    )(tokens, gain.reshape(1, -1), *weights)


def span_kernel(lengths, keys, decays, weighted, start_factor, columns):
    seq_count, channels, span = keys.shape
    place = lax.broadcasted_iota(jnp.int32, (1, span), 1)
    for n in range(seq_count):
        length = lengths[n]
        decay = decays[n]
        last = jnp.sum(jnp.where(place == length - 2, decay, 0.0), axis=1, keepdims=True)
        factor = jnp.where(place < length - 1, jnp.exp(last - decay), 0.0)
        weighted[n] = keys[n].astype(f32) * factor
        columns[:, n : n + 1] = last
    start_factor[...] = jnp.exp(columns[...].T)[:seq_count]


def span_terms(lengths, keys, decays):
    seq_count, channels, span = keys.shape
    vmem = pl.BlockSpec(memory_space=pltpu.VMEM)
    return pl.pallas_call(
        span_kernel,
        in_specs=[pl.BlockSpec(memory_space=pltpu.SMEM), vmem, vmem],
        out_shape=(
            jax.ShapeDtypeStruct(keys.shape, f32),
            jax.ShapeDtypeStruct((seq_count, channels), f32),
        ),
        scratch_shapes=[pltpu.VMEM((channels, LANES), f32)],
        name="span",
    )(lengths, keys, decays)


def attend_kernel(arrived, weighted, start_factor, values, state, bias, gain, out):
    seq_count, channels = start_factor.shape
    heads = channels // KEY_WIDTH
    width = heads * DV
    total = arrived[0].astype(f32)
    for k in range(1, arrived.shape[0]):
        total += arrived[k].astype(f32)
    query_sum = total[:, :channels]
    key_sum = total[:, channels : 2 * channels]
    decay_sum = total[:, 2 * channels : 3 * channels]
    value_sum = total[:, 3 * channels : 3 * channels + width]
    gate_sum = total[:, 3 * channels + width : 3 * channels + 2 * width]
    square = jnp.sum(total[:, 3 * channels + 2 * width :], axis=1, keepdims=True)
    scale = lax.rsqrt(square / D + NORM_EPS)
    query = query_sum * scale * KEY_WIDTH ** (-0.5)
    key_new = key_sum * scale
    value_new = value_sum * scale
    gate = gate_sum * scale
    before = decay_sum * scale + bias[...]
    log_sigmoid = jnp.minimum(before, 0.0) - jnp.log1p(jnp.exp(-jnp.abs(before)))
    decayed = query * jnp.exp(log_sigmoid / DECAY_SOFTNESS)

    key_head = lax.broadcasted_iota(jnp.int32, (SUBLANES, channels), 1) // KEY_WIDTH
    key_row = lax.broadcasted_iota(jnp.int32, (SUBLANES, channels), 0)
    value_head = lax.broadcasted_iota(jnp.int32, (SUBLANES, width), 1) // DV
    value_row = lax.broadcasted_iota(jnp.int32, (SUBLANES, width), 0)
    at_start = decayed * start_factor[...]
    padded = jnp.concatenate([decayed, jnp.zeros((LANES - seq_count, channels), f32)], axis=0)
    by_channel = padded.T
    rows = []
    for n in range(seq_count):
        product = weighted[n] * by_channel[:, n : n + 1]
        scores = [
            jnp.sum(product[h * KEY_WIDTH : (h + 1) * KEY_WIDTH], axis=0, keepdims=True)
            for h in range(heads)
        ]
        scores.append(jnp.zeros((SUBLANES - heads, product.shape[1]), f32))
        low = jnp.concatenate(scores, axis=0).astype(bf16)
        history = lax.dot_general(
            low, values[n], (((1,), (1,)), ((), ())), preferred_element_type=f32
        )
        of_heads = jnp.where(key_head == key_row, at_start[n : n + 1], 0.0)
        carried = lax.dot_general(
            of_heads,
            state[n].reshape(channels, DV),
            (((1,), (0,)), ((), ())),
            precision=lax.Precision.HIGHEST,
            preferred_element_type=f32,
        )
        both = history + jnp.concatenate([carried] * heads, axis=1)
        rows.append(jnp.sum(jnp.where(value_head == value_row, both, 0.0), axis=0, keepdims=True))
    raw = jnp.concatenate(rows, axis=0)
    match = query * key_new
    own = jnp.zeros_like(raw)
    column = lax.broadcasted_iota(jnp.int32, raw.shape, 1) // DV
    channel = lax.broadcasted_iota(jnp.int32, match.shape, 1) // KEY_WIDTH
    for h in range(heads):
        amount = jnp.sum(jnp.where(channel == h, match, 0.0), axis=1, keepdims=True)
        own = jnp.where(column == h, amount, own)
    raw = raw + own * value_new
    power = raw * raw
    inverse = jnp.zeros_like(raw)
    for h in range(heads):
        mean = jnp.sum(jnp.where(column == h, power, 0.0), axis=1, keepdims=True) / DV
        inverse = jnp.where(column == h, lax.rsqrt(mean + NORM_EPS), inverse)
    mixed = raw * inverse * gain[...] * (gate * jax.nn.sigmoid(gate))
    half = seq_count // CORES
    low = mixed.astype(bf16)
    for c in range(CORES):
        piece = low[c * half : (c + 1) * half]
        for k in range(out.shape[0] // CORES):
            out[k * CORES + c] = piece


def attend(arrived, weighted, start_factor, values, state, bias, gain):
    seq_count, width = values.shape[:2]
    half = seq_count // CORES
    return pl.pallas_call(
        attend_kernel,
        out_shape=jax.ShapeDtypeStruct((arrived.shape[0] * CORES, half, width), bf16),
        name="attend",
    )(arrived, weighted, start_factor, values, state, bias, gain)


def shards(
    tokens,
    span_lengths,
    block_state,
    key_cache,
    value_cache,
    decay_cache,
    attn_gain,
    query_weight,
    key_weight,
    value_weight,
    gate_weight,
    decay_matrix,
    decay_offset_bias,
    head_gain,
    out_weight,
    mixer_gain,
    up_weight,
    down_weight,
):
    seq_count, head_count = block_state.shape[:2]
    peers = lax.axis_size("kv")
    core = lax.axis_index("core")
    half = seq_count // CORES
    rows_half = peers * half
    values = head_count * DV

    sent = project(
        tokens, attn_gain, (query_weight, key_weight, decay_matrix, value_weight, gate_weight)
    )
    arrived = exchange(sent.reshape(peers, seq_count, -1), "kv")

    swap = [(c, CORES - 1 - c) for c in range(CORES)]
    out_other = lax.ppermute(out_weight, "core", swap)
    up_other = lax.ppermute(up_weight, "core", swap)
    down_other = lax.ppermute(down_weight, "core", swap)
    out_first = jnp.where(core == 0, out_weight, out_other)
    out_second = jnp.where(core == 0, out_other, out_weight)
    own_tokens = lax.dynamic_index_in_dim(
        tokens.reshape(peers, CORES, half, -1), core, 1, keepdims=False
    ).reshape(rows_half, -1)
    weighted, start_factor = span_terms(span_lengths, key_cache, decay_cache)
    gain = jnp.tile(head_gain, head_count).reshape(1, -1)
    (
        arrived,
        out_first,
        out_second,
        up_other,
        down_other,
        own_tokens,
        weighted,
        start_factor,
        gain,
    ) = lax.optimization_barrier(
        (
            arrived,
            out_first,
            out_second,
            up_other,
            down_other,
            own_tokens,
            weighted,
            start_factor,
            gain,
        )
    )

    spread = attend(
        arrived,
        weighted,
        start_factor,
        value_cache,
        block_state,
        decay_offset_bias.reshape(1, -1),
        gain,
    )
    heads = exchange(spread, ("kv", "core")).reshape(peers, CORES, half, values)
    attn_terms = dot(heads[:, 0].reshape(rows_half, values), out_first) + dot(
        heads[:, 1].reshape(rows_half, values), out_second
    )
    attn_out = jnp.sum(to_everyone(attn_terms.astype(bf16), "x").astype(f32), axis=0)
    resid = (own_tokens.astype(f32) + attn_out).astype(bf16)
    resid_rows = resid.astype(f32)
    mixer_square = jnp.sum(resid_rows * resid_rows, axis=1, keepdims=True)
    mixer_scaled = (resid_rows * mixer_gain).astype(bf16)
    up_sent = jnp.concatenate(
        [
            dot(mixer_scaled, up_weight).astype(bf16),
            dot(mixer_scaled, up_other).astype(bf16),
            square_lanes(mixer_square),
        ],
        axis=1,
    )
    up_total = jnp.sum(exchange(up_sent.reshape(peers, half, -1), "kv").astype(f32), axis=0)
    hidden_count = up_weight.shape[1] * CORES
    before, squares = up_total[:, :hidden_count], up_total[:, hidden_count:]
    mixer_scale = lax.rsqrt((squares[:, :1] + squares[:, 1:2]) / D + NORM_EPS)
    hidden = jnp.square(jax.nn.relu(before * mixer_scale)).astype(bf16)
    every = to_everyone(hidden, "kv").reshape(rows_half, hidden_count)
    own_count = up_weight.shape[1]
    down_terms = dot(every[:, :own_count], down_weight) + dot(every[:, own_count:], down_other)
    mixer_out = jnp.sum(to_everyone(down_terms.astype(bf16), "x").astype(f32), axis=0)
    own_out = (resid_rows + mixer_out).astype(bf16)
    both = to_everyone(own_out, "core").reshape(CORES, peers, half, -1)
    return jnp.swapaxes(both, 0, 1).reshape(peers * seq_count, -1)


def solution(mesh):
    sizes = dict(mesh.shape)
    fine = Mesh(
        mesh.devices.reshape(sizes["grp"], sizes["kv"], sizes["tp"] // CORES, CORES),
        ("grp", "kv", "x", "core"),
    )
    tp = ("x", "core")
    placed = (
        P("grp", "kv"),
        P(("grp", "kv")),
        P(("grp", "kv"), tp, None, None),
        P(("grp", "kv"), tp, None),
        P(("grp", "kv"), tp, None),
        P(("grp", "kv"), tp, None),
        P("kv"),
        P("kv", tp),
        P("kv", tp),
        P("kv", tp),
        P("kv", tp),
        P("kv", tp),
        P(tp),
        P(),
        P(tp, "kv"),
        P("kv"),
        P("kv", tp),
        P(tp, "kv"),
    )
    return jax.shard_map(
        shards, mesh=fine, in_specs=placed, out_specs=P("grp", "kv"), check_vma=False
    )
```

```python
import jax
import jax.numpy as jnp
from jax import lax
from jax.experimental import pallas as pl
from jax.experimental.pallas import tpu as pltpu
from jax.sharding import Mesh, PartitionSpec as P

D = 4096
KEY_WIDTH = 32
DV = 64
LANES = 128
SUBLANES = 8
CORES = 2

NORM_EPS = 1e-06
DECAY_SOFTNESS = 16.0

f32, bf16 = jnp.float32, jnp.bfloat16


def exchange(pieces, axes):
    return lax.all_to_all(pieces, axes, 0, 0, tiled=True)


def to_everyone(value, axes):
    peers = lax.axis_size(axes)
    return exchange(jnp.broadcast_to(value[None], (peers, *value.shape)), axes)


def in_vmem(*values):
    return tuple(pltpu.with_memory_space_constraint(v, pltpu.VMEM) for v in values)


VMEM = pl.BlockSpec(memory_space=pltpu.VMEM)


def dot(a, b):
    return jnp.dot(a, b, preferred_element_type=f32)


def project_kernel(tokens, gain, *refs):
    *weights, out = refs
    rows = tokens[...].astype(f32)
    square = jnp.sum(rows * rows, axis=1, keepdims=True)
    scaled = (rows * gain[...]).astype(bf16)
    start = 0
    for w in weights:
        width = w.shape[1]
        out[:, start : start + width] = dot(scaled, w[...]).astype(bf16)
        start += width
    high = square.astype(bf16).astype(f32)
    lane = lax.broadcasted_iota(jnp.int32, (rows.shape[0], LANES), 1)
    out[:, start:] = jnp.where(lane == 0, high, jnp.where(lane == 1, square - high, 0.0)).astype(
        bf16
    )


def project(tokens, gain, weights):
    width = sum(w.shape[1] for w in weights) + LANES
    return pl.pallas_call(
        project_kernel,
        out_shape=jax.ShapeDtypeStruct((tokens.shape[0], width), bf16),
        name="project",
    )(tokens, gain.reshape(1, -1), *weights)


def span_kernel(
    lengths, keys, decays, head_gain, bias, wide_gain, weighted, start_factor, *small_and_columns
):
    head_gain_out, bias_out, wide_gain_out, columns = small_and_columns
    head_gain_out[...] = jnp.concatenate(
        [head_gain[...]] * (head_gain_out.shape[1] // head_gain.shape[1]), axis=1
    )
    bias_out[...] = bias[...]
    wide_gain_out[...] = wide_gain[...]
    seq_count, channels, span = keys.shape
    place = lax.broadcasted_iota(jnp.int32, (1, span), 1)
    for n in range(seq_count):
        length = lengths[n]
        decay = decays[n]
        last = jnp.sum(jnp.where(place == length - 2, decay, 0.0), axis=1, keepdims=True)
        factor = jnp.where(place < length - 1, jnp.exp(last - decay), 0.0)
        weighted[n] = keys[n].astype(f32) * factor
        columns[:, n : n + 1] = last
    start_factor[...] = jnp.exp(columns[...].T)[:seq_count]


def span_terms(lengths, keys, decays, head_gain, bias, wide_gain):
    seq_count, channels, span = keys.shape
    values = channels // KEY_WIDTH * DV
    return pl.pallas_call(
        span_kernel,
        in_specs=[pl.BlockSpec(memory_space=pltpu.SMEM)] + [VMEM] * 5,
        out_specs=(VMEM,) * 5,
        out_shape=(
            pltpu.VMEM(keys.shape, f32),
            pltpu.VMEM((seq_count, channels), f32),
            pltpu.VMEM((1, values), f32),
            pltpu.VMEM((1, channels), f32),
            pltpu.VMEM((1, wide_gain.shape[0]), f32),
        ),
        scratch_shapes=[pltpu.VMEM((channels, LANES), f32)],
        compiler_params=pltpu.CompilerParams(vmem_limit_bytes=16 << 20),
        name="span",
    )(lengths, keys, decays, *(v.reshape(1, -1) for v in (head_gain, bias, wide_gain)))


def attend_kernel(arrived, weighted, start_factor, bias, gain, values, state, out):
    seq_count, channels = start_factor.shape
    heads = channels // KEY_WIDTH
    width = heads * DV
    total = arrived[0].astype(f32)
    for k in range(1, arrived.shape[0]):
        total += arrived[k].astype(f32)
    query_sum = total[:, :channels]
    key_sum = total[:, channels : 2 * channels]
    decay_sum = total[:, 2 * channels : 3 * channels]
    value_sum = total[:, 3 * channels : 3 * channels + width]
    gate_sum = total[:, 3 * channels + width : 3 * channels + 2 * width]
    square = jnp.sum(total[:, 3 * channels + 2 * width :], axis=1, keepdims=True)
    scale = lax.rsqrt(square / D + NORM_EPS)
    query = query_sum * scale * KEY_WIDTH ** (-0.5)
    key_new = key_sum * scale
    value_new = value_sum * scale
    gate = gate_sum * scale
    before = decay_sum * scale + bias[...]
    log_sigmoid = jnp.minimum(before, 0.0) - jnp.log1p(jnp.exp(-jnp.abs(before)))
    decayed = query * jnp.exp(log_sigmoid / DECAY_SOFTNESS)

    key_head = lax.broadcasted_iota(jnp.int32, (SUBLANES, channels), 1) // KEY_WIDTH
    key_row = lax.broadcasted_iota(jnp.int32, (SUBLANES, channels), 0)
    value_head = lax.broadcasted_iota(jnp.int32, (SUBLANES, width), 1) // DV
    value_row = lax.broadcasted_iota(jnp.int32, (SUBLANES, width), 0)
    at_start = decayed * start_factor[...]
    padded = jnp.concatenate([decayed, jnp.zeros((LANES - seq_count, channels), f32)], axis=0)
    by_channel = padded.T
    rows = []
    for n in range(seq_count):
        product = weighted[n] * by_channel[:, n : n + 1]
        scores = [
            jnp.sum(product[h * KEY_WIDTH : (h + 1) * KEY_WIDTH], axis=0, keepdims=True)
            for h in range(heads)
        ]
        scores.append(jnp.zeros((SUBLANES - heads, product.shape[1]), f32))
        low = jnp.concatenate(scores, axis=0).astype(bf16)
        history = lax.dot_general(
            low, values[n], (((1,), (1,)), ((), ())), preferred_element_type=f32
        )
        of_heads = jnp.where(key_head == key_row, at_start[n : n + 1], 0.0)
        carried = lax.dot_general(
            of_heads,
            state[n].reshape(channels, DV),
            (((1,), (0,)), ((), ())),
            precision=lax.Precision.HIGHEST,
            preferred_element_type=f32,
        )
        both = history + jnp.concatenate([carried] * heads, axis=1)
        rows.append(jnp.sum(jnp.where(value_head == value_row, both, 0.0), axis=0, keepdims=True))
    raw = jnp.concatenate(rows, axis=0)
    match = query * key_new
    own = jnp.zeros_like(raw)
    column = lax.broadcasted_iota(jnp.int32, raw.shape, 1) // DV
    channel = lax.broadcasted_iota(jnp.int32, match.shape, 1) // KEY_WIDTH
    for h in range(heads):
        amount = jnp.sum(jnp.where(channel == h, match, 0.0), axis=1, keepdims=True)
        own = jnp.where(column == h, amount, own)
    raw = raw + own * value_new
    power = raw * raw
    inverse = jnp.zeros_like(raw)
    for h in range(heads):
        mean = jnp.sum(jnp.where(column == h, power, 0.0), axis=1, keepdims=True) / DV
        inverse = jnp.where(column == h, lax.rsqrt(mean + NORM_EPS), inverse)
    mixed = raw * inverse * gain[...] * (gate * jax.nn.sigmoid(gate))
    half = seq_count // CORES
    low = mixed.astype(bf16)
    for c in range(CORES):
        piece = low[c * half : (c + 1) * half]
        for k in range(out.shape[0] // CORES):
            out[k * CORES + c] = piece


def attend(arrived, weighted, start_factor, values, state, bias, gain):
    seq_count, width = values.shape[:2]
    half = seq_count // CORES
    return pl.pallas_call(
        attend_kernel,
        in_specs=[VMEM] * 7,
        out_specs=VMEM,
        out_shape=pltpu.VMEM((arrived.shape[0] * CORES, half, width), bf16),
        compiler_params=pltpu.CompilerParams(vmem_limit_bytes=16 << 20),
        name="attend",
    )(*in_vmem(arrived, weighted, start_factor, bias, gain, values, state))


def hidden_kernel(arrived, tokens, gain, first, second_far, out, resid, second, done):
    copy = pltpu.make_async_copy(second_far, second, done)
    copy.start()
    total = arrived[0].astype(f32)
    for x in range(1, arrived.shape[0]):
        total += arrived[x].astype(f32)
    low = (tokens[...].astype(f32) + total).astype(bf16)
    resid[...] = low
    rows = low.astype(f32)
    square = jnp.sum(rows * rows, axis=1, keepdims=True)
    scaled = (rows * gain[...]).astype(bf16)
    own = first.shape[1]
    high = square.astype(bf16).astype(f32)
    lane = lax.broadcasted_iota(jnp.int32, (rows.shape[0], LANES), 1)
    squares = jnp.where(lane == 0, high, jnp.where(lane == 1, square - high, 0.0)).astype(bf16)
    pieces, half = out.shape[:2]


    def put(at, value):
        for k in range(pieces):
            out[k, :, at : at + value.shape[1]] = value[k * half : (k + 1) * half]

    put(0, dot(scaled, first[...]).astype(bf16))
    put(2 * own, squares)
    copy.wait()
    put(own, dot(scaled, second[...]).astype(bf16))


def hidden_terms(arrived, tokens, gain, first, second, peers):
    rows, width = tokens.shape
    return pl.pallas_call(
        hidden_kernel,
        in_specs=[VMEM] * 4 + [pl.BlockSpec(memory_space=pl.ANY)],
        out_specs=(VMEM, VMEM),
        out_shape=(
            pltpu.VMEM((peers, rows // peers, 2 * first.shape[1] + LANES), bf16),
            pltpu.VMEM((rows, width), bf16),
        ),
        scratch_shapes=[pltpu.VMEM(second.shape, second.dtype), pltpu.SemaphoreType.DMA(())],
        compiler_params=pltpu.CompilerParams(vmem_limit_bytes=16 << 20),
        name="hidden",
    )(*in_vmem(arrived, tokens, gain, first), second)


def shards(
    tokens,
    span_lengths,
    block_state,
    key_cache,
    value_cache,
    decay_cache,
    attn_gain,
    query_weight,
    key_weight,
    value_weight,
    gate_weight,
    decay_matrix,
    decay_offset_bias,
    head_gain,
    out_weight,
    mixer_gain,
    up_weight,
    down_weight,
):
    seq_count, head_count = block_state.shape[:2]
    peers = lax.axis_size("kv")
    core = lax.axis_index("core")
    half = seq_count // CORES
    rows_half = peers * half
    values = head_count * DV

    sent = project(
        tokens, attn_gain, (query_weight, key_weight, decay_matrix, value_weight, gate_weight)
    )
    arrived = exchange(sent.reshape(peers, seq_count, -1), "kv")

    swap = [(c, CORES - 1 - c) for c in range(CORES)]
    out_other = lax.ppermute(out_weight, "core", swap)
    up_other = lax.ppermute(up_weight, "core", swap)
    down_other = lax.ppermute(down_weight, "core", swap)
    out_first = jnp.where(core == 0, out_weight, out_other)
    out_second = jnp.where(core == 0, out_other, out_weight)
    own_tokens = lax.dynamic_index_in_dim(
        tokens.reshape(peers, CORES, half, -1), core, 1, keepdims=False
    ).reshape(rows_half, -1)
    ready = span_terms(
        span_lengths, key_cache, decay_cache, head_gain, decay_offset_bias, mixer_gain
    )
    arrived, out_first, out_second, up_other, down_other, own_tokens, ready = (
        lax.optimization_barrier(
            (arrived, out_first, out_second, up_other, down_other, own_tokens, ready)
        )
    )
    weighted, start_factor, gain, bias, wide_gain = ready

    spread = attend(arrived, weighted, start_factor, value_cache, block_state, bias, gain)
    heads = exchange(spread, ("kv", "core")).reshape(peers, CORES, half, values)
    attn_terms = dot(heads[:, 0].reshape(rows_half, values), out_first) + dot(
        heads[:, 1].reshape(rows_half, values), out_second
    )
    attn_arrived = to_everyone(attn_terms.astype(bf16), "x")
    up_sent, resid = hidden_terms(
        attn_arrived, own_tokens, wide_gain, up_weight, up_other, peers
    )
    up_total = jnp.sum(exchange(up_sent, "kv").astype(f32), axis=0)
    hidden_count = up_weight.shape[1] * CORES
    before, squares = up_total[:, :hidden_count], up_total[:, hidden_count:]
    mixer_scale = lax.rsqrt((squares[:, :1] + squares[:, 1:2]) / D + NORM_EPS)
    hidden = jnp.square(jax.nn.relu(before * mixer_scale)).astype(bf16)
    every = to_everyone(hidden, "kv").reshape(rows_half, hidden_count)
    own_count = up_weight.shape[1]
    down_terms = dot(every[:, :own_count], down_weight) + dot(every[:, own_count:], down_other)
    mixer_out = jnp.sum(to_everyone(down_terms.astype(bf16), "x").astype(f32), axis=0)
    own_out = (resid.astype(f32) + mixer_out).astype(bf16)
    both = to_everyone(own_out, "core").reshape(CORES, peers, half, -1)
    return jnp.swapaxes(both, 0, 1).reshape(peers * seq_count, -1)


def solution(mesh):
    sizes = dict(mesh.shape)
    fine = Mesh(
        mesh.devices.reshape(sizes["grp"], sizes["kv"], sizes["tp"] // CORES, CORES),
        ("grp", "kv", "x", "core"),
    )
    tp = ("x", "core")
    placed = (
        P("grp", "kv"),
        P(("grp", "kv")),
        P(("grp", "kv"), tp, None, None),
        P(("grp", "kv"), tp, None),
        P(("grp", "kv"), tp, None),
        P(("grp", "kv"), tp, None),
        P("kv"),
        P("kv", tp),
        P("kv", tp),
        P("kv", tp),
        P("kv", tp),
        P("kv", tp),
        P(tp),
        P(),
        P(tp, "kv"),
        P("kv"),
        P("kv", tp),
        P(tp, "kv"),
    )
    return jax.shard_map(
        shards, mesh=fine, in_specs=placed, out_specs=P("grp", "kv"), check_vma=False
    )
```

```python
import jax
import jax.numpy as jnp
from jax import lax
from jax.experimental import pallas as pl
from jax.experimental.pallas import tpu as pltpu
from jax.sharding import Mesh, PartitionSpec as P

D = 4096
KEY_WIDTH = 32
DV = 64
LANES = 128
SUBLANES = 8
CORES = 2

NORM_EPS = 1e-06
DECAY_SOFTNESS = 16.0

f32, bf16 = jnp.float32, jnp.bfloat16


def exchange(pieces, axes):
    return lax.all_to_all(pieces, axes, 0, 0, tiled=True)


def to_everyone(value, axes):
    peers = lax.axis_size(axes)
    return exchange(jnp.broadcast_to(value[None], (peers, *value.shape)), axes)


def in_vmem(*values):
    return tuple(pltpu.with_memory_space_constraint(v, pltpu.VMEM) for v in values)


VMEM = pl.BlockSpec(memory_space=pltpu.VMEM)
ANY = pl.BlockSpec(memory_space=pl.ANY)


def dot(a, b):
    return jnp.dot(a, b, preferred_element_type=f32)


def project_kernel(tokens, gain, *refs):
    *weights, out = refs
    rows = tokens[...].astype(f32)
    square = jnp.sum(rows * rows, axis=1, keepdims=True)
    scaled = (rows * gain[...]).astype(bf16)
    start = 0
    for w in weights:
        width = w.shape[1]
        out[:, start : start + width] = dot(scaled, w[...]).astype(bf16)
        start += width
    high = square.astype(bf16).astype(f32)
    lane = lax.broadcasted_iota(jnp.int32, (rows.shape[0], LANES), 1)
    out[:, start:] = jnp.where(lane == 0, high, jnp.where(lane == 1, square - high, 0.0)).astype(
        bf16
    )


def project(tokens, gain, weights):
    width = sum(w.shape[1] for w in weights) + LANES
    return pl.pallas_call(
        project_kernel,
        out_shape=jax.ShapeDtypeStruct((tokens.shape[0], width), bf16),
        name="project",
    )(tokens, gain.reshape(1, -1), *weights)


def span_kernel(
    lengths, keys, decays, head_gain, bias, wide_gain, weighted, start_factor, *small_and_columns
):
    head_gain_out, bias_out, wide_gain_out, columns = small_and_columns
    head_gain_out[...] = jnp.concatenate(
        [head_gain[...]] * (head_gain_out.shape[1] // head_gain.shape[1]), axis=1
    )
    bias_out[...] = bias[...]
    wide_gain_out[...] = wide_gain[...]
    seq_count, channels, span = keys.shape
    place = lax.broadcasted_iota(jnp.int32, (1, span), 1)
    for n in range(seq_count):
        length = lengths[n]
        decay = decays[n]
        last = jnp.sum(jnp.where(place == length - 2, decay, 0.0), axis=1, keepdims=True)
        factor = jnp.where(place < length - 1, jnp.exp(last - decay), 0.0)
        weighted[n] = keys[n].astype(f32) * factor
        columns[:, n : n + 1] = last
    start_factor[...] = jnp.exp(columns[...].T)[:seq_count]


def span_terms(lengths, keys, decays, head_gain, bias, wide_gain):
    seq_count, channels, span = keys.shape
    values = channels // KEY_WIDTH * DV
    return pl.pallas_call(
        span_kernel,
        in_specs=[pl.BlockSpec(memory_space=pltpu.SMEM)] + [VMEM] * 5,
        out_specs=(VMEM,) * 5,
        out_shape=(
            pltpu.VMEM(keys.shape, f32),
            pltpu.VMEM((seq_count, channels), f32),
            pltpu.VMEM((1, values), f32),
            pltpu.VMEM((1, channels), f32),
            pltpu.VMEM((1, wide_gain.shape[0]), f32),
        ),
        scratch_shapes=[pltpu.VMEM((channels, LANES), f32)],
        compiler_params=pltpu.CompilerParams(vmem_limit_bytes=16 << 20),
        name="span",
    )(lengths, keys, decays, *(v.reshape(1, -1) for v in (head_gain, bias, wide_gain)))


def attend_kernel(arrived, weighted, start_factor, bias, gain, values, state, *refs):
    count = len(refs) // 2 - 1
    far, (out, *near, done) = refs[:count], refs[count:]
    copies = [
        pltpu.make_async_copy(a, b, done.at[i]) for i, (a, b) in enumerate(zip(far, near))
    ]
    for copy in copies:
        copy.start()
    seq_count, channels = start_factor.shape
    heads = channels // KEY_WIDTH
    width = heads * DV
    total = arrived[0].astype(f32)
    for k in range(1, arrived.shape[0]):
        total += arrived[k].astype(f32)
    query_sum = total[:, :channels]
    key_sum = total[:, channels : 2 * channels]
    decay_sum = total[:, 2 * channels : 3 * channels]
    value_sum = total[:, 3 * channels : 3 * channels + width]
    gate_sum = total[:, 3 * channels + width : 3 * channels + 2 * width]
    square = jnp.sum(total[:, 3 * channels + 2 * width :], axis=1, keepdims=True)
    scale = lax.rsqrt(square / D + NORM_EPS)
    query = query_sum * scale * KEY_WIDTH ** (-0.5)
    key_new = key_sum * scale
    value_new = value_sum * scale
    gate = gate_sum * scale
    before = decay_sum * scale + bias[...]
    log_sigmoid = jnp.minimum(before, 0.0) - jnp.log1p(jnp.exp(-jnp.abs(before)))
    decayed = query * jnp.exp(log_sigmoid / DECAY_SOFTNESS)

    key_head = lax.broadcasted_iota(jnp.int32, (SUBLANES, channels), 1) // KEY_WIDTH
    key_row = lax.broadcasted_iota(jnp.int32, (SUBLANES, channels), 0)
    value_head = lax.broadcasted_iota(jnp.int32, (SUBLANES, width), 1) // DV
    value_row = lax.broadcasted_iota(jnp.int32, (SUBLANES, width), 0)
    at_start = decayed * start_factor[...]
    padded = jnp.concatenate([decayed, jnp.zeros((LANES - seq_count, channels), f32)], axis=0)
    by_channel = padded.T
    rows = []
    for n in range(seq_count):
        product = weighted[n] * by_channel[:, n : n + 1]
        scores = [
            jnp.sum(product[h * KEY_WIDTH : (h + 1) * KEY_WIDTH], axis=0, keepdims=True)
            for h in range(heads)
        ]
        scores.append(jnp.zeros((SUBLANES - heads, product.shape[1]), f32))
        low = jnp.concatenate(scores, axis=0).astype(bf16)
        history = lax.dot_general(
            low, values[n], (((1,), (1,)), ((), ())), preferred_element_type=f32
        )
        of_heads = jnp.where(key_head == key_row, at_start[n : n + 1], 0.0)
        carried = lax.dot_general(
            of_heads,
            state[n].reshape(channels, DV),
            (((1,), (0,)), ((), ())),
            precision=lax.Precision.HIGHEST,
            preferred_element_type=f32,
        )
        both = history + jnp.concatenate([carried] * heads, axis=1)
        rows.append(jnp.sum(jnp.where(value_head == value_row, both, 0.0), axis=0, keepdims=True))
    raw = jnp.concatenate(rows, axis=0)
    match = query * key_new
    own = jnp.zeros_like(raw)
    column = lax.broadcasted_iota(jnp.int32, raw.shape, 1) // DV
    channel = lax.broadcasted_iota(jnp.int32, match.shape, 1) // KEY_WIDTH
    for h in range(heads):
        amount = jnp.sum(jnp.where(channel == h, match, 0.0), axis=1, keepdims=True)
        own = jnp.where(column == h, amount, own)
    raw = raw + own * value_new
    power = raw * raw
    inverse = jnp.zeros_like(raw)
    for h in range(heads):
        mean = jnp.sum(jnp.where(column == h, power, 0.0), axis=1, keepdims=True) / DV
        inverse = jnp.where(column == h, lax.rsqrt(mean + NORM_EPS), inverse)
    mixed = raw * inverse * gain[...] * (gate * jax.nn.sigmoid(gate))
    half = seq_count // CORES
    low = mixed.astype(bf16)
    for c in range(CORES):
        piece = low[c * half : (c + 1) * half]
        for k in range(out.shape[0] // CORES):
            out[k * CORES + c] = piece
    for copy in copies:
        copy.wait()


def attend(arrived, weighted, start_factor, values, state, bias, gain, shards_far):
    seq_count, width = values.shape[:2]
    half = seq_count // CORES
    count = len(shards_far)
    return pl.pallas_call(
        attend_kernel,
        in_specs=[VMEM] * 7 + [ANY] * count,
        out_specs=(VMEM,) * (1 + count),
        out_shape=(
            pltpu.VMEM((arrived.shape[0] * CORES, half, width), bf16),
            *(pltpu.VMEM(v.shape, v.dtype) for v in shards_far),
        ),
        scratch_shapes=[pltpu.SemaphoreType.DMA((count,))],
        compiler_params=pltpu.CompilerParams(vmem_limit_bytes=16 << 20),
        name="attend",
    )(*in_vmem(arrived, weighted, start_factor, bias, gain, values, state), *shards_far)


def hidden_kernel(
    arrived, tokens, gain, first, second_far, shard_far, out, resid, shard, second, done
):
    second_copy = pltpu.make_async_copy(second_far, second, done.at[0])
    second_copy.start()
    shard_copy = pltpu.make_async_copy(shard_far, shard, done.at[1])
    shard_copy.start()
    total = arrived[0].astype(f32)
    for x in range(1, arrived.shape[0]):
        total += arrived[x].astype(f32)
    low = (tokens[...].astype(f32) + total).astype(bf16)
    resid[...] = low
    rows = low.astype(f32)
    square = jnp.sum(rows * rows, axis=1, keepdims=True)
    scaled = (rows * gain[...]).astype(bf16)
    own = first.shape[1]
    high = square.astype(bf16).astype(f32)
    lane = lax.broadcasted_iota(jnp.int32, (rows.shape[0], LANES), 1)
    squares = jnp.where(lane == 0, high, jnp.where(lane == 1, square - high, 0.0)).astype(bf16)
    pieces, half = out.shape[:2]


    def put(at, value):
        for k in range(pieces):
            out[k, :, at : at + value.shape[1]] = value[k * half : (k + 1) * half]

    put(0, dot(scaled, first[...]).astype(bf16))
    put(2 * own, squares)
    second_copy.wait()
    put(own, dot(scaled, second[...]).astype(bf16))
    shard_copy.wait()


def hidden_terms(arrived, tokens, gain, first, second, shard, peers):
    rows, width = tokens.shape
    return pl.pallas_call(
        hidden_kernel,
        in_specs=[VMEM] * 4 + [ANY] * 2,
        out_specs=(VMEM,) * 3,
        out_shape=(
            pltpu.VMEM((peers, rows // peers, 2 * first.shape[1] + LANES), bf16),
            pltpu.VMEM((rows, width), bf16),
            pltpu.VMEM(shard.shape, shard.dtype),
        ),
        scratch_shapes=[
            pltpu.VMEM(second.shape, second.dtype),
            pltpu.SemaphoreType.DMA((2,)),
        ],
        compiler_params=pltpu.CompilerParams(vmem_limit_bytes=16 << 20),
        name="hidden",
    )(*in_vmem(arrived, tokens, gain, first), second, shard)


def active_kernel(arrived, out):
    count = out.shape[2]
    total = arrived[0].astype(f32)
    for k in range(1, arrived.shape[0]):
        total += arrived[k].astype(f32)
    square = jnp.sum(total[:, count:], axis=1, keepdims=True)
    before = total[:, :count] * lax.rsqrt(square / D + NORM_EPS)
    up = jnp.maximum(before, 0.0)
    low = (up * up).astype(bf16)
    for k in range(out.shape[0]):
        out[k] = low


def active(arrived):
    pieces, rows, width = arrived.shape
    return pl.pallas_call(
        active_kernel,
        in_specs=[VMEM],
        out_specs=VMEM,
        out_shape=pltpu.VMEM((pieces, rows, width - LANES), bf16),
        compiler_params=pltpu.CompilerParams(vmem_limit_bytes=8 << 20),
        name="active",
    )(*in_vmem(arrived))


def shards(
    tokens,
    span_lengths,
    block_state,
    key_cache,
    value_cache,
    decay_cache,
    attn_gain,
    query_weight,
    key_weight,
    value_weight,
    gate_weight,
    decay_matrix,
    decay_offset_bias,
    head_gain,
    out_weight,
    mixer_gain,
    up_weight,
    down_weight,
):
    seq_count, head_count = block_state.shape[:2]
    peers = lax.axis_size("kv")
    core = lax.axis_index("core")
    half = seq_count // CORES
    rows_half = peers * half
    values = head_count * DV

    sent = project(
        tokens, attn_gain, (query_weight, key_weight, decay_matrix, value_weight, gate_weight)
    )
    arrived = exchange(sent.reshape(peers, seq_count, -1), "kv")

    swap = [(c, CORES - 1 - c) for c in range(CORES)]
    out_other = lax.ppermute(out_weight, "core", swap)
    up_other = lax.ppermute(up_weight, "core", swap)
    down_other = lax.ppermute(down_weight, "core", swap)
    out_first = jnp.where(core == 0, out_weight, out_other)
    out_second = jnp.where(core == 0, out_other, out_weight)
    own_tokens = lax.dynamic_index_in_dim(
        tokens.reshape(peers, CORES, half, -1), core, 1, keepdims=False
    ).reshape(rows_half, -1)
    ready = span_terms(
        span_lengths, key_cache, decay_cache, head_gain, decay_offset_bias, mixer_gain
    )
    arrived, out_first, out_second, up_other, down_other, own_tokens, ready = (
        lax.optimization_barrier(
            (arrived, out_first, out_second, up_other, down_other, own_tokens, ready)
        )
    )
    weighted, start_factor, gain, bias, wide_gain = ready

    spread, out_first, out_second = attend(
        arrived,
        weighted,
        start_factor,
        value_cache,
        block_state,
        bias,
        gain,
        (out_first, out_second),
    )
    heads = exchange(spread, ("kv", "core")).reshape(peers, CORES, half, values)
    attn_terms = dot(heads[:, 0].reshape(rows_half, values), out_first) + dot(
        heads[:, 1].reshape(rows_half, values), out_second
    )
    attn_arrived = to_everyone(attn_terms.astype(bf16), "x")
    up_sent, resid, down_other = hidden_terms(
        attn_arrived, own_tokens, wide_gain, up_weight, up_other, down_other, peers
    )
    hidden = active(exchange(up_sent, "kv"))
    every = exchange(hidden, "kv").reshape(rows_half, -1)
    own_count = up_weight.shape[1]
    down_terms = dot(every[:, :own_count], down_weight) + dot(every[:, own_count:], down_other)
    mixer_out = jnp.sum(to_everyone(down_terms.astype(bf16), "x").astype(f32), axis=0)
    own_out = (resid.astype(f32) + mixer_out).astype(bf16)
    other_out = lax.ppermute(own_out, "core", swap)
    low_half = jnp.where(core == 0, own_out, other_out).reshape(peers, half, -1)
    high_half = jnp.where(core == 0, other_out, own_out).reshape(peers, half, -1)
    return jnp.concatenate([low_half, high_half], axis=1).reshape(peers * seq_count, -1)


def solution(mesh):
    sizes = dict(mesh.shape)
    fine = Mesh(
        mesh.devices.reshape(sizes["grp"], sizes["kv"], sizes["tp"] // CORES, CORES),
        ("grp", "kv", "x", "core"),
    )
    tp = ("x", "core")
    placed = (
        P("grp", "kv"),
        P(("grp", "kv")),
        P(("grp", "kv"), tp, None, None),
        P(("grp", "kv"), tp, None),
        P(("grp", "kv"), tp, None),
        P(("grp", "kv"), tp, None),
        P("kv"),
        P("kv", tp),
        P("kv", tp),
        P("kv", tp),
        P("kv", tp),
        P("kv", tp),
        P(tp),
        P(),
        P(tp, "kv"),
        P("kv"),
        P("kv", tp),
        P(tp, "kv"),
    )
    return jax.shard_map(
        shards, mesh=fine, in_specs=placed, out_specs=P("grp", "kv"), check_vma=False
    )
```

```python
import jax
import jax.numpy as jnp
from jax import lax
from jax.experimental import pallas as pl
from jax.experimental.pallas import tpu as pltpu
from jax.sharding import Mesh, PartitionSpec as P

D = 4096
KEY_WIDTH = 32
DV = 64
LANES = 128
SUBLANES = 8
CORES = 2
STAGGER_NS = 4500

NORM_EPS = 1e-06
DECAY_SOFTNESS = 16.0

f32, bf16 = jnp.float32, jnp.bfloat16


def exchange(pieces, axes):
    return lax.all_to_all(pieces, axes, 0, 0, tiled=True)


def to_everyone(value, axes):
    peers = lax.axis_size(axes)
    return exchange(jnp.broadcast_to(value[None], (peers, *value.shape)), axes)


def in_vmem(*values):
    return tuple(pltpu.with_memory_space_constraint(v, pltpu.VMEM) for v in values)


VMEM = pl.BlockSpec(memory_space=pltpu.VMEM)
ANY = pl.BlockSpec(memory_space=pl.ANY)


def dot(a, b):
    return jnp.dot(a, b, preferred_element_type=f32)


def project_kernel(tokens, gain, *refs):
    *weights, out = refs
    rows = tokens[...].astype(f32)
    square = jnp.sum(rows * rows, axis=1, keepdims=True)
    scaled = (rows * gain[...]).astype(bf16)
    start = 0
    for w in weights:
        width = w.shape[1]
        out[:, start : start + width] = dot(scaled, w[...]).astype(bf16)
        start += width
    high = square.astype(bf16).astype(f32)
    lane = lax.broadcasted_iota(jnp.int32, (rows.shape[0], LANES), 1)
    out[:, start:] = jnp.where(lane == 0, high, jnp.where(lane == 1, square - high, 0.0)).astype(
        bf16
    )


def project(tokens, gain, weights):
    width = sum(w.shape[1] for w in weights) + LANES
    return pl.pallas_call(
        project_kernel,
        out_shape=jax.ShapeDtypeStruct((tokens.shape[0], width), bf16),
        name="project",
    )(tokens, gain.reshape(1, -1), *weights)


def span_kernel(
    lengths, keys, decays, head_gain, bias, wide_gain, weighted, start_factor, *small_and_columns
):
    head_gain_out, bias_out, wide_gain_out, columns = small_and_columns
    head_gain_out[...] = jnp.concatenate(
        [head_gain[...]] * (head_gain_out.shape[1] // head_gain.shape[1]), axis=1
    )
    bias_out[...] = bias[...]
    wide_gain_out[...] = wide_gain[...]
    seq_count, channels, span = keys.shape
    place = lax.broadcasted_iota(jnp.int32, (1, span), 1)
    for n in range(seq_count):
        length = lengths[n]
        decay = decays[n]
        last = jnp.sum(jnp.where(place == length - 2, decay, 0.0), axis=1, keepdims=True)
        factor = jnp.where(place < length - 1, jnp.exp(last - decay), 0.0)
        weighted[n] = keys[n].astype(f32) * factor
        columns[:, n : n + 1] = last
    start_factor[...] = jnp.exp(columns[...].T)[:seq_count]


def span_terms(lengths, keys, decays, head_gain, bias, wide_gain):
    seq_count, channels, span = keys.shape
    values = channels // KEY_WIDTH * DV
    return pl.pallas_call(
        span_kernel,
        in_specs=[pl.BlockSpec(memory_space=pltpu.SMEM)] + [VMEM] * 5,
        out_specs=(VMEM,) * 5,
        out_shape=(
            pltpu.VMEM(keys.shape, f32),
            pltpu.VMEM((seq_count, channels), f32),
            pltpu.VMEM((1, values), f32),
            pltpu.VMEM((1, channels), f32),
            pltpu.VMEM((1, wide_gain.shape[0]), f32),
        ),
        scratch_shapes=[pltpu.VMEM((channels, LANES), f32)],
        compiler_params=pltpu.CompilerParams(vmem_limit_bytes=16 << 20),
        name="span",
    )(lengths, keys, decays, *(v.reshape(1, -1) for v in (head_gain, bias, wide_gain)))


def attend_kernel(arrived, weighted, start_factor, bias, gain, values, state, *refs):
    count = len(refs) // 2 - 1
    far, (out, *near, done) = refs[:count], refs[count:]
    copies = [
        pltpu.make_async_copy(a, b, done.at[i]) for i, (a, b) in enumerate(zip(far, near))
    ]
    for copy in copies:
        copy.start()
    seq_count, channels = start_factor.shape
    heads = channels // KEY_WIDTH
    width = heads * DV
    total = arrived[0].astype(f32)
    for k in range(1, arrived.shape[0]):
        total += arrived[k].astype(f32)
    query_sum = total[:, :channels]
    key_sum = total[:, channels : 2 * channels]
    decay_sum = total[:, 2 * channels : 3 * channels]
    value_sum = total[:, 3 * channels : 3 * channels + width]
    gate_sum = total[:, 3 * channels + width : 3 * channels + 2 * width]
    square = jnp.sum(total[:, 3 * channels + 2 * width :], axis=1, keepdims=True)
    scale = lax.rsqrt(square / D + NORM_EPS)
    query = query_sum * scale * KEY_WIDTH ** (-0.5)
    key_new = key_sum * scale
    value_new = value_sum * scale
    gate = gate_sum * scale
    before = decay_sum * scale + bias[...]
    log_sigmoid = jnp.minimum(before, 0.0) - jnp.log1p(jnp.exp(-jnp.abs(before)))
    decayed = query * jnp.exp(log_sigmoid / DECAY_SOFTNESS)

    key_head = lax.broadcasted_iota(jnp.int32, (SUBLANES, channels), 1) // KEY_WIDTH
    key_row = lax.broadcasted_iota(jnp.int32, (SUBLANES, channels), 0)
    value_head = lax.broadcasted_iota(jnp.int32, (SUBLANES, width), 1) // DV
    value_row = lax.broadcasted_iota(jnp.int32, (SUBLANES, width), 0)
    at_start = decayed * start_factor[...]
    padded = jnp.concatenate([decayed, jnp.zeros((LANES - seq_count, channels), f32)], axis=0)
    by_channel = padded.T
    rows = []
    for n in range(seq_count):
        product = weighted[n] * by_channel[:, n : n + 1]
        scores = [
            jnp.sum(product[h * KEY_WIDTH : (h + 1) * KEY_WIDTH], axis=0, keepdims=True)
            for h in range(heads)
        ]
        scores.append(jnp.zeros((SUBLANES - heads, product.shape[1]), f32))
        low = jnp.concatenate(scores, axis=0).astype(bf16)
        history = lax.dot_general(
            low, values[n], (((1,), (1,)), ((), ())), preferred_element_type=f32
        )
        of_heads = jnp.where(key_head == key_row, at_start[n : n + 1], 0.0)
        carried = lax.dot_general(
            of_heads,
            state[n].reshape(channels, DV),
            (((1,), (0,)), ((), ())),
            precision=lax.Precision.HIGHEST,
            preferred_element_type=f32,
        )
        both = history + jnp.concatenate([carried] * heads, axis=1)
        rows.append(jnp.sum(jnp.where(value_head == value_row, both, 0.0), axis=0, keepdims=True))
    raw = jnp.concatenate(rows, axis=0)
    match = query * key_new
    own = jnp.zeros_like(raw)
    column = lax.broadcasted_iota(jnp.int32, raw.shape, 1) // DV
    channel = lax.broadcasted_iota(jnp.int32, match.shape, 1) // KEY_WIDTH
    for h in range(heads):
        amount = jnp.sum(jnp.where(channel == h, match, 0.0), axis=1, keepdims=True)
        own = jnp.where(column == h, amount, own)
    raw = raw + own * value_new
    power = raw * raw
    inverse = jnp.zeros_like(raw)
    for h in range(heads):
        mean = jnp.sum(jnp.where(column == h, power, 0.0), axis=1, keepdims=True) / DV
        inverse = jnp.where(column == h, lax.rsqrt(mean + NORM_EPS), inverse)
    mixed = raw * inverse * gain[...] * (gate * jax.nn.sigmoid(gate))
    half = seq_count // CORES
    low = mixed.astype(bf16)
    for c in range(CORES):
        piece = low[c * half : (c + 1) * half]
        for k in range(out.shape[0] // CORES):
            out[k * CORES + c] = piece
    for copy in copies:
        copy.wait()


def attend(arrived, weighted, start_factor, values, state, bias, gain, shards_far):
    seq_count, width = values.shape[:2]
    half = seq_count // CORES
    count = len(shards_far)
    return pl.pallas_call(
        attend_kernel,
        in_specs=[VMEM] * 7 + [ANY] * count,
        out_specs=(VMEM,) * (1 + count),
        out_shape=(
            pltpu.VMEM((arrived.shape[0] * CORES, half, width), bf16),
            *(pltpu.VMEM(v.shape, v.dtype) for v in shards_far),
        ),
        scratch_shapes=[pltpu.SemaphoreType.DMA((count,))],
        compiler_params=pltpu.CompilerParams(vmem_limit_bytes=16 << 20),
        name="attend",
    )(*in_vmem(arrived, weighted, start_factor, bias, gain, values, state), *shards_far)


def merge_kernel(heads_first, heads_second, first, second, out):
    @pl.when(lax.axis_index("core") == 0)
    def fall_behind():
        pl.delay(STAGGER_NS)

    terms = dot(heads_first[...], first[...]) + dot(heads_second[...], second[...])
    low = terms.astype(bf16)
    for x in range(out.shape[0]):
        out[x] = low


def merge(heads_first, heads_second, first, second, peers):
    shape = (peers, heads_first.shape[0], first.shape[1])
    return pl.pallas_call(
        merge_kernel,
        in_specs=[VMEM] * 4,
        out_specs=VMEM,
        out_shape=pltpu.VMEM(shape, bf16),
        compiler_params=pltpu.CompilerParams(vmem_limit_bytes=8 << 20),
        name="merge",
    )(*in_vmem(heads_first, heads_second, first, second))


def hidden_kernel(
    arrived, tokens, gain, first, second_far, shard_far, out, resid, shard, second, done
):
    second_copy = pltpu.make_async_copy(second_far, second, done.at[0])
    second_copy.start()
    shard_copy = pltpu.make_async_copy(shard_far, shard, done.at[1])
    shard_copy.start()
    total = arrived[0].astype(f32)
    for x in range(1, arrived.shape[0]):
        total += arrived[x].astype(f32)
    low = (tokens[...].astype(f32) + total).astype(bf16)
    resid[...] = low
    rows = low.astype(f32)
    square = jnp.sum(rows * rows, axis=1, keepdims=True)
    scaled = (rows * gain[...]).astype(bf16)
    own = first.shape[1]
    high = square.astype(bf16).astype(f32)
    lane = lax.broadcasted_iota(jnp.int32, (rows.shape[0], LANES), 1)
    squares = jnp.where(lane == 0, high, jnp.where(lane == 1, square - high, 0.0)).astype(bf16)
    pieces, half = out.shape[:2]


    def put(at, value):
        for k in range(pieces):
            out[k, :, at : at + value.shape[1]] = value[k * half : (k + 1) * half]

    put(0, dot(scaled, first[...]).astype(bf16))
    put(2 * own, squares)
    second_copy.wait()
    put(own, dot(scaled, second[...]).astype(bf16))
    shard_copy.wait()


def hidden_terms(arrived, tokens, gain, first, second, shard, peers):
    rows, width = tokens.shape
    return pl.pallas_call(
        hidden_kernel,
        in_specs=[VMEM] * 4 + [ANY] * 2,
        out_specs=(VMEM,) * 3,
        out_shape=(
            pltpu.VMEM((peers, rows // peers, 2 * first.shape[1] + LANES), bf16),
            pltpu.VMEM((rows, width), bf16),
            pltpu.VMEM(shard.shape, shard.dtype),
        ),
        scratch_shapes=[
            pltpu.VMEM(second.shape, second.dtype),
            pltpu.SemaphoreType.DMA((2,)),
        ],
        compiler_params=pltpu.CompilerParams(vmem_limit_bytes=16 << 20),
        name="hidden",
    )(*in_vmem(arrived, tokens, gain, first), second, shard)


def active_kernel(arrived, out):
    count = out.shape[2]
    total = arrived[0].astype(f32)
    for k in range(1, arrived.shape[0]):
        total += arrived[k].astype(f32)
    square = jnp.sum(total[:, count:], axis=1, keepdims=True)
    before = total[:, :count] * lax.rsqrt(square / D + NORM_EPS)
    up = jnp.maximum(before, 0.0)
    low = (up * up).astype(bf16)
    for k in range(out.shape[0]):
        out[k] = low


def active(arrived):
    pieces, rows, width = arrived.shape
    return pl.pallas_call(
        active_kernel,
        in_specs=[VMEM],
        out_specs=VMEM,
        out_shape=pltpu.VMEM((pieces, rows, width - LANES), bf16),
        compiler_params=pltpu.CompilerParams(vmem_limit_bytes=8 << 20),
        name="active",
    )(*in_vmem(arrived))


def shards(
    tokens,
    span_lengths,
    block_state,
    key_cache,
    value_cache,
    decay_cache,
    attn_gain,
    query_weight,
    key_weight,
    value_weight,
    gate_weight,
    decay_matrix,
    decay_offset_bias,
    head_gain,
    out_weight,
    mixer_gain,
    up_weight,
    down_weight,
):
    seq_count, head_count = block_state.shape[:2]
    peers = lax.axis_size("kv")
    core = lax.axis_index("core")
    half = seq_count // CORES
    rows_half = peers * half
    values = head_count * DV

    sent = project(
        tokens, attn_gain, (query_weight, key_weight, decay_matrix, value_weight, gate_weight)
    )
    arrived = exchange(sent.reshape(peers, seq_count, -1), "kv")

    swap = [(c, CORES - 1 - c) for c in range(CORES)]
    out_other = lax.ppermute(out_weight, "core", swap)
    up_other = lax.ppermute(up_weight, "core", swap)
    down_other = lax.ppermute(down_weight, "core", swap)
    out_first = jnp.where(core == 0, out_weight, out_other)
    out_second = jnp.where(core == 0, out_other, out_weight)
    own_tokens = lax.dynamic_index_in_dim(
        tokens.reshape(peers, CORES, half, -1), core, 1, keepdims=False
    ).reshape(rows_half, -1)
    ready = span_terms(
        span_lengths, key_cache, decay_cache, head_gain, decay_offset_bias, mixer_gain
    )
    arrived, out_first, out_second, up_other, down_other, own_tokens, ready = (
        lax.optimization_barrier(
            (arrived, out_first, out_second, up_other, down_other, own_tokens, ready)
        )
    )
    weighted, start_factor, gain, bias, wide_gain = ready

    spread, out_first, out_second = attend(
        arrived,
        weighted,
        start_factor,
        value_cache,
        block_state,
        bias,
        gain,
        (out_first, out_second),
    )
    heads = exchange(spread, ("kv", "core")).reshape(peers, CORES, half, values)
    attn_terms = merge(
        heads[:, 0].reshape(rows_half, values),
        heads[:, 1].reshape(rows_half, values),
        out_first,
        out_second,
        lax.axis_size("x"),
    )
    attn_arrived = exchange(attn_terms, "x")
    up_sent, resid, down_other = hidden_terms(
        attn_arrived, own_tokens, wide_gain, up_weight, up_other, down_other, peers
    )
    hidden = active(exchange(up_sent, "kv"))
    every = exchange(hidden, "kv").reshape(rows_half, -1)
    own_count = up_weight.shape[1]
    down_terms = dot(every[:, :own_count], down_weight) + dot(every[:, own_count:], down_other)
    mixer_out = jnp.sum(to_everyone(down_terms.astype(bf16), "x").astype(f32), axis=0)
    own_out = (resid.astype(f32) + mixer_out).astype(bf16)
    other_out = lax.ppermute(own_out, "core", swap)
    low_half = jnp.where(core == 0, own_out, other_out).reshape(peers, half, -1)
    high_half = jnp.where(core == 0, other_out, own_out).reshape(peers, half, -1)
    return jnp.concatenate([low_half, high_half], axis=1).reshape(peers * seq_count, -1)


def solution(mesh):
    sizes = dict(mesh.shape)
    fine = Mesh(
        mesh.devices.reshape(sizes["grp"], sizes["kv"], sizes["tp"] // CORES, CORES),
        ("grp", "kv", "x", "core"),
    )
    tp = ("x", "core")
    placed = (
        P("grp", "kv"),
        P(("grp", "kv")),
        P(("grp", "kv"), tp, None, None),
        P(("grp", "kv"), tp, None),
        P(("grp", "kv"), tp, None),
        P(("grp", "kv"), tp, None),
        P("kv"),
        P("kv", tp),
        P("kv", tp),
        P("kv", tp),
        P("kv", tp),
        P("kv", tp),
        P(tp),
        P(),
        P(tp, "kv"),
        P("kv"),
        P("kv", tp),
        P(tp, "kv"),
    )
    return jax.shard_map(
        shards, mesh=fine, in_specs=placed, out_specs=P("grp", "kv"), check_vma=False
    )
```

```python
import jax
import jax.numpy as jnp
from jax import lax
from jax.experimental import pallas as pl
from jax.experimental.pallas import tpu as pltpu
from jax.sharding import Mesh, PartitionSpec as P

D = 4096
KEY_WIDTH = 32
DV = 64
LANES = 128
SUBLANES = 8
CORES = 2
STAGGER_NS = 5600

NORM_EPS = 1e-06
DECAY_SOFTNESS = 16.0

f32, bf16 = jnp.float32, jnp.bfloat16


def exchange(pieces, axes):
    return lax.all_to_all(pieces, axes, 0, 0, tiled=True)


def to_everyone(value, axes):
    peers = lax.axis_size(axes)
    return exchange(jnp.broadcast_to(value[None], (peers, *value.shape)), axes)


def in_vmem(*values):
    return tuple(pltpu.with_memory_space_constraint(v, pltpu.VMEM) for v in values)


VMEM = pl.BlockSpec(memory_space=pltpu.VMEM)
ANY = pl.BlockSpec(memory_space=pl.ANY)


def dot(a, b):
    return jnp.dot(a, b, preferred_element_type=f32)


def project_kernel(tokens, gain, *refs):
    *weights, out = refs
    rows = tokens[...].astype(f32)
    square = jnp.sum(rows * rows, axis=1, keepdims=True)
    scaled = (rows * gain[...]).astype(bf16)
    start = 0
    for w in weights:
        width = w.shape[1]
        out[:, start : start + width] = dot(scaled, w[...]).astype(bf16)
        start += width
    high = square.astype(bf16).astype(f32)
    lane = lax.broadcasted_iota(jnp.int32, (rows.shape[0], LANES), 1)
    out[:, start:] = jnp.where(lane == 0, high, jnp.where(lane == 1, square - high, 0.0)).astype(
        bf16
    )


def project(tokens, gain, weights):
    width = sum(w.shape[1] for w in weights) + LANES
    return pl.pallas_call(
        project_kernel,
        out_shape=jax.ShapeDtypeStruct((tokens.shape[0], width), bf16),
        name="project",
    )(tokens, gain.reshape(1, -1), *weights)


def span_kernel(
    lengths, keys, decays, head_gain, bias, wide_gain, weighted, start_factor, *small_and_columns
):
    head_gain_out, bias_out, wide_gain_out, columns = small_and_columns
    head_gain_out[...] = jnp.concatenate(
        [head_gain[...]] * (head_gain_out.shape[1] // head_gain.shape[1]), axis=1
    )
    bias_out[...] = bias[...]
    wide_gain_out[...] = wide_gain[...]
    seq_count, channels, span = keys.shape
    place = lax.broadcasted_iota(jnp.int32, (1, span), 1)
    for n in range(seq_count):
        length = lengths[n]
        decay = decays[n]
        last = jnp.sum(jnp.where(place == length - 2, decay, 0.0), axis=1, keepdims=True)
        factor = jnp.where(place < length - 1, jnp.exp(last - decay), 0.0)
        weighted[n] = keys[n].astype(f32) * factor
        columns[:, n : n + 1] = last
    start_factor[...] = jnp.exp(columns[...].T)[:seq_count]


def span_terms(lengths, keys, decays, head_gain, bias, wide_gain):
    seq_count, channels, span = keys.shape
    values = channels // KEY_WIDTH * DV
    return pl.pallas_call(
        span_kernel,
        in_specs=[pl.BlockSpec(memory_space=pltpu.SMEM)] + [VMEM] * 5,
        out_specs=(VMEM,) * 5,
        out_shape=(
            pltpu.VMEM(keys.shape, f32),
            pltpu.VMEM((seq_count, channels), f32),
            pltpu.VMEM((1, values), f32),
            pltpu.VMEM((1, channels), f32),
            pltpu.VMEM((1, wide_gain.shape[0]), f32),
        ),
        scratch_shapes=[pltpu.VMEM((channels, LANES), f32)],
        compiler_params=pltpu.CompilerParams(vmem_limit_bytes=16 << 20),
        name="span",
    )(lengths, keys, decays, *(v.reshape(1, -1) for v in (head_gain, bias, wide_gain)))


def attend_kernel(arrived, weighted, start_factor, bias, gain, values, state, *refs):
    count = len(refs) // 2 - 1
    far, (out, *near, done) = refs[:count], refs[count:]
    copies = [
        pltpu.make_async_copy(a, b, done.at[i]) for i, (a, b) in enumerate(zip(far, near))
    ]
    for copy in copies:
        copy.start()
    seq_count, channels = start_factor.shape
    heads = channels // KEY_WIDTH
    width = heads * DV
    total = arrived[0].astype(f32)
    for k in range(1, arrived.shape[0]):
        total += arrived[k].astype(f32)
    query_sum = total[:, :channels]
    key_sum = total[:, channels : 2 * channels]
    decay_sum = total[:, 2 * channels : 3 * channels]
    value_sum = total[:, 3 * channels : 3 * channels + width]
    gate_sum = total[:, 3 * channels + width : 3 * channels + 2 * width]
    square = jnp.sum(total[:, 3 * channels + 2 * width :], axis=1, keepdims=True)
    scale = lax.rsqrt(square / D + NORM_EPS)
    query = query_sum * scale * KEY_WIDTH ** (-0.5)
    key_new = key_sum * scale
    value_new = value_sum * scale
    gate = gate_sum * scale
    before = decay_sum * scale + bias[...]
    log_sigmoid = jnp.minimum(before, 0.0) - jnp.log1p(jnp.exp(-jnp.abs(before)))
    decayed = query * jnp.exp(log_sigmoid / DECAY_SOFTNESS)

    key_head = lax.broadcasted_iota(jnp.int32, (SUBLANES, channels), 1) // KEY_WIDTH
    key_row = lax.broadcasted_iota(jnp.int32, (SUBLANES, channels), 0)
    value_head = lax.broadcasted_iota(jnp.int32, (SUBLANES, width), 1) // DV
    value_row = lax.broadcasted_iota(jnp.int32, (SUBLANES, width), 0)
    at_start = decayed * start_factor[...]
    padded = jnp.concatenate([decayed, jnp.zeros((LANES - seq_count, channels), f32)], axis=0)
    by_channel = padded.T
    rows = []
    for n in range(seq_count):
        product = weighted[n] * by_channel[:, n : n + 1]
        scores = [
            jnp.sum(product[h * KEY_WIDTH : (h + 1) * KEY_WIDTH], axis=0, keepdims=True)
            for h in range(heads)
        ]
        scores.append(jnp.zeros((SUBLANES - heads, product.shape[1]), f32))
        low = jnp.concatenate(scores, axis=0).astype(bf16)
        history = lax.dot_general(
            low, values[n], (((1,), (1,)), ((), ())), preferred_element_type=f32
        )
        of_heads = jnp.where(key_head == key_row, at_start[n : n + 1], 0.0)
        carried = lax.dot_general(
            of_heads,
            state[n].reshape(channels, DV),
            (((1,), (0,)), ((), ())),
            precision=lax.Precision.HIGHEST,
            preferred_element_type=f32,
        )
        both = history + jnp.concatenate([carried] * heads, axis=1)
        rows.append(jnp.sum(jnp.where(value_head == value_row, both, 0.0), axis=0, keepdims=True))
    raw = jnp.concatenate(rows, axis=0)
    match = query * key_new
    own = jnp.zeros_like(raw)
    column = lax.broadcasted_iota(jnp.int32, raw.shape, 1) // DV
    channel = lax.broadcasted_iota(jnp.int32, match.shape, 1) // KEY_WIDTH
    for h in range(heads):
        amount = jnp.sum(jnp.where(channel == h, match, 0.0), axis=1, keepdims=True)
        own = jnp.where(column == h, amount, own)
    raw = raw + own * value_new
    power = raw * raw
    inverse = jnp.zeros_like(raw)
    for h in range(heads):
        mean = jnp.sum(jnp.where(column == h, power, 0.0), axis=1, keepdims=True) / DV
        inverse = jnp.where(column == h, lax.rsqrt(mean + NORM_EPS), inverse)
    mixed = raw * inverse * gain[...] * (gate * jax.nn.sigmoid(gate))
    half = seq_count // CORES
    low = mixed.astype(bf16)
    for c in range(CORES):
        piece = low[c * half : (c + 1) * half]
        for k in range(out.shape[0] // CORES):
            out[k * CORES + c] = piece
    for copy in copies:
        copy.wait()


def attend(arrived, weighted, start_factor, values, state, bias, gain, shards_far):
    seq_count, width = values.shape[:2]
    half = seq_count // CORES
    count = len(shards_far)
    return pl.pallas_call(
        attend_kernel,
        in_specs=[VMEM] * 7 + [ANY] * count,
        out_specs=(VMEM,) * (1 + count),
        out_shape=(
            pltpu.VMEM((arrived.shape[0] * CORES, half, width), bf16),
            *(pltpu.VMEM(v.shape, v.dtype) for v in shards_far),
        ),
        scratch_shapes=[pltpu.SemaphoreType.DMA((count,))],
        compiler_params=pltpu.CompilerParams(vmem_limit_bytes=16 << 20),
        name="attend",
    )(*in_vmem(arrived, weighted, start_factor, bias, gain, values, state), *shards_far)


def merge_kernel(heads_first, heads_second, first, second, out):
    @pl.when(lax.axis_index("core") == 0)
    def fall_behind():
        pl.delay(STAGGER_NS)

    terms = dot(heads_first[...], first[...]) + dot(heads_second[...], second[...])
    low = terms.astype(bf16)
    for x in range(out.shape[0]):
        out[x] = low


def merge(heads_first, heads_second, first, second, peers):
    shape = (peers, heads_first.shape[0], first.shape[1])
    return pl.pallas_call(
        merge_kernel,
        in_specs=[VMEM] * 4,
        out_specs=VMEM,
        out_shape=pltpu.VMEM(shape, bf16),
        compiler_params=pltpu.CompilerParams(vmem_limit_bytes=8 << 20),
        name="merge",
    )(*in_vmem(heads_first, heads_second, first, second))


def hidden_kernel(
    arrived, tokens, gain, first, second_far, shard_far, out, resid, shard, second, done
):
    second_copy = pltpu.make_async_copy(second_far, second, done.at[0])
    second_copy.start()
    shard_copy = pltpu.make_async_copy(shard_far, shard, done.at[1])
    shard_copy.start()
    total = arrived[0].astype(f32)
    for x in range(1, arrived.shape[0]):
        total += arrived[x].astype(f32)
    low = (tokens[...].astype(f32) + total).astype(bf16)
    resid[...] = low
    rows = low.astype(f32)
    square = jnp.sum(rows * rows, axis=1, keepdims=True)
    scaled = (rows * gain[...]).astype(bf16)
    own = first.shape[1]
    high = square.astype(bf16).astype(f32)
    lane = lax.broadcasted_iota(jnp.int32, (rows.shape[0], LANES), 1)
    squares = jnp.where(lane == 0, high, jnp.where(lane == 1, square - high, 0.0)).astype(bf16)
    pieces, half = out.shape[:2]


    def put(at, value):
        for k in range(pieces):
            out[k, :, at : at + value.shape[1]] = value[k * half : (k + 1) * half]

    put(0, dot(scaled, first[...]).astype(bf16))
    put(2 * own, squares)
    second_copy.wait()
    put(own, dot(scaled, second[...]).astype(bf16))
    shard_copy.wait()


def hidden_terms(arrived, tokens, gain, first, second, shard, peers):
    rows, width = tokens.shape
    return pl.pallas_call(
        hidden_kernel,
        in_specs=[VMEM] * 4 + [ANY] * 2,
        out_specs=(VMEM,) * 3,
        out_shape=(
            pltpu.VMEM((peers, rows // peers, 2 * first.shape[1] + LANES), bf16),
            pltpu.VMEM((rows, width), bf16),
            pltpu.VMEM(shard.shape, shard.dtype),
        ),
        scratch_shapes=[
            pltpu.VMEM(second.shape, second.dtype),
            pltpu.SemaphoreType.DMA((2,)),
        ],
        compiler_params=pltpu.CompilerParams(vmem_limit_bytes=16 << 20),
        name="hidden",
    )(*in_vmem(arrived, tokens, gain, first), second, shard)


def active_kernel(arrived, out):
    count = out.shape[2]
    total = arrived[0].astype(f32)
    for k in range(1, arrived.shape[0]):
        total += arrived[k].astype(f32)
    square = jnp.sum(total[:, count:], axis=1, keepdims=True)
    before = total[:, :count] * lax.rsqrt(square / D + NORM_EPS)
    up = jnp.maximum(before, 0.0)
    low = (up * up).astype(bf16)
    for k in range(out.shape[0]):
        out[k] = low


def active(arrived):
    pieces, rows, width = arrived.shape
    return pl.pallas_call(
        active_kernel,
        in_specs=[VMEM],
        out_specs=VMEM,
        out_shape=pltpu.VMEM((pieces, rows, width - LANES), bf16),
        compiler_params=pltpu.CompilerParams(vmem_limit_bytes=8 << 20),
        name="active",
    )(*in_vmem(arrived))


def shards(
    tokens,
    span_lengths,
    block_state,
    key_cache,
    value_cache,
    decay_cache,
    attn_gain,
    query_weight,
    key_weight,
    value_weight,
    gate_weight,
    decay_matrix,
    decay_offset_bias,
    head_gain,
    out_weight,
    mixer_gain,
    up_weight,
    down_weight,
):
    seq_count, head_count = block_state.shape[:2]
    peers = lax.axis_size("kv")
    core = lax.axis_index("core")
    half = seq_count // CORES
    rows_half = peers * half
    values = head_count * DV

    sent = project(
        tokens, attn_gain, (query_weight, key_weight, decay_matrix, value_weight, gate_weight)
    )
    arrived = exchange(sent.reshape(peers, seq_count, -1), "kv")

    swap = [(c, CORES - 1 - c) for c in range(CORES)]
    out_other = lax.ppermute(out_weight, "core", swap)
    up_other = lax.ppermute(up_weight, "core", swap)
    down_other = lax.ppermute(down_weight, "core", swap)
    out_first = jnp.where(core == 0, out_weight, out_other)
    out_second = jnp.where(core == 0, out_other, out_weight)
    own_tokens = lax.dynamic_index_in_dim(
        tokens.reshape(peers, CORES, half, -1), core, 1, keepdims=False
    ).reshape(rows_half, -1)
    ready = span_terms(
        span_lengths, key_cache, decay_cache, head_gain, decay_offset_bias, mixer_gain
    )
    arrived, out_first, out_second, up_other, down_other, own_tokens, ready = (
        lax.optimization_barrier(
            (arrived, out_first, out_second, up_other, down_other, own_tokens, ready)
        )
    )
    weighted, start_factor, gain, bias, wide_gain = ready

    spread, out_first, out_second = attend(
        arrived,
        weighted,
        start_factor,
        value_cache,
        block_state,
        bias,
        gain,
        (out_first, out_second),
    )
    heads = exchange(spread, ("kv", "core")).reshape(peers, CORES, half, values)
    attn_terms = merge(
        heads[:, 0].reshape(rows_half, values),
        heads[:, 1].reshape(rows_half, values),
        out_first,
        out_second,
        lax.axis_size("x"),
    )
    attn_arrived = exchange(attn_terms, "x")
    up_sent, resid, down_other = hidden_terms(
        attn_arrived, own_tokens, wide_gain, up_weight, up_other, down_other, peers
    )
    hidden = active(exchange(up_sent, "kv"))
    every = exchange(hidden, "kv").reshape(rows_half, -1)
    own_count = up_weight.shape[1]
    down_terms = dot(every[:, :own_count], down_weight) + dot(every[:, own_count:], down_other)
    mixer_out = jnp.sum(to_everyone(down_terms.astype(bf16), "x").astype(f32), axis=0)
    own_out = (resid.astype(f32) + mixer_out).astype(bf16)
    other_out = lax.ppermute(own_out, "core", swap)
    low_half = jnp.where(core == 0, own_out, other_out).reshape(peers, half, -1)
    high_half = jnp.where(core == 0, other_out, own_out).reshape(peers, half, -1)
    return jnp.concatenate([low_half, high_half], axis=1).reshape(peers * seq_count, -1)


def solution(mesh):
    sizes = dict(mesh.shape)
    fine = Mesh(
        mesh.devices.reshape(sizes["grp"], sizes["kv"], sizes["tp"] // CORES, CORES),
        ("grp", "kv", "x", "core"),
    )
    tp = ("x", "core")
    placed = (
        P("grp", "kv"),
        P(("grp", "kv")),
        P(("grp", "kv"), tp, None, None),
        P(("grp", "kv"), tp, None),
        P(("grp", "kv"), tp, None),
        P(("grp", "kv"), tp, None),
        P("kv"),
        P("kv", tp),
        P("kv", tp),
        P("kv", tp),
        P("kv", tp),
        P("kv", tp),
        P(tp),
        P(),
        P(tp, "kv"),
        P("kv"),
        P("kv", tp),
        P(tp, "kv"),
    )
    return jax.shard_map(
        shards, mesh=fine, in_specs=placed, out_specs=P("grp", "kv"), check_vma=False
    )
```

```python
import jax
import jax.numpy as jnp
from jax import lax
from jax.experimental import pallas as pl
from jax.experimental.pallas import tpu as pltpu
from jax.sharding import Mesh, PartitionSpec as P

D = 4096
KEY_WIDTH = 32
DV = 64
LANES = 128
SUBLANES = 8
CORES = 2
STAGGER_NS = 3500

NORM_EPS = 1e-06
DECAY_SOFTNESS = 16.0

f32, bf16 = jnp.float32, jnp.bfloat16


def exchange(pieces, axes):
    return lax.all_to_all(pieces, axes, 0, 0, tiled=True)


def to_everyone(value, axes):
    peers = lax.axis_size(axes)
    return exchange(jnp.broadcast_to(value[None], (peers, *value.shape)), axes)


def in_vmem(*values):
    return tuple(pltpu.with_memory_space_constraint(v, pltpu.VMEM) for v in values)


VMEM = pl.BlockSpec(memory_space=pltpu.VMEM)
ANY = pl.BlockSpec(memory_space=pl.ANY)


def dot(a, b):
    return jnp.dot(a, b, preferred_element_type=f32)


def project_kernel(tokens, gain, *refs):
    *weights, out = refs
    rows = tokens[...].astype(f32)
    square = jnp.sum(rows * rows, axis=1, keepdims=True)
    scaled = (rows * gain[...]).astype(bf16)
    start = 0
    for w in weights:
        width = w.shape[1]
        out[:, start : start + width] = dot(scaled, w[...]).astype(bf16)
        start += width
    high = square.astype(bf16).astype(f32)
    lane = lax.broadcasted_iota(jnp.int32, (rows.shape[0], LANES), 1)
    out[:, start:] = jnp.where(lane == 0, high, jnp.where(lane == 1, square - high, 0.0)).astype(
        bf16
    )


def project(tokens, gain, weights):
    width = sum(w.shape[1] for w in weights) + LANES
    return pl.pallas_call(
        project_kernel,
        out_shape=jax.ShapeDtypeStruct((tokens.shape[0], width), bf16),
        name="project",
    )(tokens, gain.reshape(1, -1), *weights)


def span_kernel(
    lengths, keys, decays, head_gain, bias, wide_gain, weighted, start_factor, *small_and_columns
):
    head_gain_out, bias_out, wide_gain_out, columns = small_and_columns
    head_gain_out[...] = jnp.concatenate(
        [head_gain[...]] * (head_gain_out.shape[1] // head_gain.shape[1]), axis=1
    )
    bias_out[...] = bias[...]
    wide_gain_out[...] = wide_gain[...]
    seq_count, channels, span = keys.shape
    place = lax.broadcasted_iota(jnp.int32, (1, span), 1)
    for n in range(seq_count):
        length = lengths[n]
        decay = decays[n]
        last = jnp.sum(jnp.where(place == length - 2, decay, 0.0), axis=1, keepdims=True)
        factor = jnp.where(place < length - 1, jnp.exp(last - decay), 0.0)
        weighted[n] = keys[n].astype(f32) * factor
        columns[:, n : n + 1] = last
    start_factor[...] = jnp.exp(columns[...].T)[:seq_count]


def span_terms(lengths, keys, decays, head_gain, bias, wide_gain):
    seq_count, channels, span = keys.shape
    values = channels // KEY_WIDTH * DV
    return pl.pallas_call(
        span_kernel,
        in_specs=[pl.BlockSpec(memory_space=pltpu.SMEM)] + [VMEM] * 5,
        out_specs=(VMEM,) * 5,
        out_shape=(
            pltpu.VMEM(keys.shape, f32),
            pltpu.VMEM((seq_count, channels), f32),
            pltpu.VMEM((1, values), f32),
            pltpu.VMEM((1, channels), f32),
            pltpu.VMEM((1, wide_gain.shape[0]), f32),
        ),
        scratch_shapes=[pltpu.VMEM((channels, LANES), f32)],
        compiler_params=pltpu.CompilerParams(vmem_limit_bytes=16 << 20),
        name="span",
    )(lengths, keys, decays, *(v.reshape(1, -1) for v in (head_gain, bias, wide_gain)))


def attend_kernel(arrived, weighted, start_factor, bias, gain, values, state, *refs):
    count = len(refs) // 2 - 1
    far, (out, *near, done) = refs[:count], refs[count:]
    copies = [
        pltpu.make_async_copy(a, b, done.at[i]) for i, (a, b) in enumerate(zip(far, near))
    ]
    for copy in copies:
        copy.start()
    seq_count, channels = start_factor.shape
    heads = channels // KEY_WIDTH
    width = heads * DV
    total = arrived[0].astype(f32)
    for k in range(1, arrived.shape[0]):
        total += arrived[k].astype(f32)
    query_sum = total[:, :channels]
    key_sum = total[:, channels : 2 * channels]
    decay_sum = total[:, 2 * channels : 3 * channels]
    value_sum = total[:, 3 * channels : 3 * channels + width]
    gate_sum = total[:, 3 * channels + width : 3 * channels + 2 * width]
    square = jnp.sum(total[:, 3 * channels + 2 * width :], axis=1, keepdims=True)
    scale = lax.rsqrt(square / D + NORM_EPS)
    query = query_sum * scale * KEY_WIDTH ** (-0.5)
    key_new = key_sum * scale
    value_new = value_sum * scale
    gate = gate_sum * scale
    before = decay_sum * scale + bias[...]
    log_sigmoid = jnp.minimum(before, 0.0) - jnp.log1p(jnp.exp(-jnp.abs(before)))
    decayed = query * jnp.exp(log_sigmoid / DECAY_SOFTNESS)

    key_head = lax.broadcasted_iota(jnp.int32, (SUBLANES, channels), 1) // KEY_WIDTH
    key_row = lax.broadcasted_iota(jnp.int32, (SUBLANES, channels), 0)
    value_head = lax.broadcasted_iota(jnp.int32, (SUBLANES, width), 1) // DV
    value_row = lax.broadcasted_iota(jnp.int32, (SUBLANES, width), 0)
    at_start = decayed * start_factor[...]
    padded = jnp.concatenate([decayed, jnp.zeros((LANES - seq_count, channels), f32)], axis=0)
    by_channel = padded.T
    rows = []
    for n in range(seq_count):
        product = weighted[n] * by_channel[:, n : n + 1]
        scores = [
            jnp.sum(product[h * KEY_WIDTH : (h + 1) * KEY_WIDTH], axis=0, keepdims=True)
            for h in range(heads)
        ]
        scores.append(jnp.zeros((SUBLANES - heads, product.shape[1]), f32))
        low = jnp.concatenate(scores, axis=0).astype(bf16)
        history = lax.dot_general(
            low, values[n], (((1,), (1,)), ((), ())), preferred_element_type=f32
        )
        of_heads = jnp.where(key_head == key_row, at_start[n : n + 1], 0.0)
        carried = lax.dot_general(
            of_heads,
            state[n].reshape(channels, DV),
            (((1,), (0,)), ((), ())),
            precision=lax.Precision.HIGHEST,
            preferred_element_type=f32,
        )
        both = history + jnp.concatenate([carried] * heads, axis=1)
        rows.append(jnp.sum(jnp.where(value_head == value_row, both, 0.0), axis=0, keepdims=True))
    raw = jnp.concatenate(rows, axis=0)
    match = query * key_new
    own = jnp.zeros_like(raw)
    column = lax.broadcasted_iota(jnp.int32, raw.shape, 1) // DV
    channel = lax.broadcasted_iota(jnp.int32, match.shape, 1) // KEY_WIDTH
    for h in range(heads):
        amount = jnp.sum(jnp.where(channel == h, match, 0.0), axis=1, keepdims=True)
        own = jnp.where(column == h, amount, own)
    raw = raw + own * value_new
    power = raw * raw
    inverse = jnp.zeros_like(raw)
    for h in range(heads):
        mean = jnp.sum(jnp.where(column == h, power, 0.0), axis=1, keepdims=True) / DV
        inverse = jnp.where(column == h, lax.rsqrt(mean + NORM_EPS), inverse)
    mixed = raw * inverse * gain[...] * (gate * jax.nn.sigmoid(gate))
    half = seq_count // CORES
    low = mixed.astype(bf16)
    for c in range(CORES):
        piece = low[c * half : (c + 1) * half]
        pieces = out.shape[0] // CORES
        for k in range(pieces):
            out[c * pieces + k] = piece
    for copy in copies:
        copy.wait()


def attend(arrived, weighted, start_factor, values, state, bias, gain, shards_far):
    seq_count, width = values.shape[:2]
    half = seq_count // CORES
    count = len(shards_far)
    return pl.pallas_call(
        attend_kernel,
        in_specs=[VMEM] * 7 + [ANY] * count,
        out_specs=(VMEM,) * (1 + count),
        out_shape=(
            pltpu.VMEM((arrived.shape[0] * CORES, half, width), bf16),
            *(pltpu.VMEM(v.shape, v.dtype) for v in shards_far),
        ),
        scratch_shapes=[pltpu.SemaphoreType.DMA((count,))],
        compiler_params=pltpu.CompilerParams(vmem_limit_bytes=16 << 20),
        name="attend",
    )(*in_vmem(arrived, weighted, start_factor, bias, gain, values, state), *shards_far)


def merge_kernel(heads_first, heads_second, first, second, out):
    @pl.when(lax.axis_index("core") == 0)
    def fall_behind():
        pl.delay(STAGGER_NS)

    terms = dot(heads_first[...], first[...]) + dot(heads_second[...], second[...])
    low = terms.astype(bf16)
    for x in range(out.shape[0]):
        out[x] = low


def merge(heads_first, heads_second, first, second, peers):
    shape = (peers, heads_first.shape[0], first.shape[1])
    return pl.pallas_call(
        merge_kernel,
        in_specs=[VMEM] * 4,
        out_specs=VMEM,
        out_shape=pltpu.VMEM(shape, bf16),
        compiler_params=pltpu.CompilerParams(vmem_limit_bytes=8 << 20),
        name="merge",
    )(*in_vmem(heads_first, heads_second, first, second))


def hidden_kernel(
    arrived, tokens, gain, first, second_far, shard_far, out, resid, shard, second, done
):
    second_copy = pltpu.make_async_copy(second_far, second, done.at[0])
    second_copy.start()
    shard_copy = pltpu.make_async_copy(shard_far, shard, done.at[1])
    shard_copy.start()
    total = arrived[0].astype(f32)
    for x in range(1, arrived.shape[0]):
        total += arrived[x].astype(f32)
    low = (tokens[...].astype(f32) + total).astype(bf16)
    resid[...] = low
    rows = low.astype(f32)
    square = jnp.sum(rows * rows, axis=1, keepdims=True)
    scaled = (rows * gain[...]).astype(bf16)
    own = first.shape[1]
    high = square.astype(bf16).astype(f32)
    lane = lax.broadcasted_iota(jnp.int32, (rows.shape[0], LANES), 1)
    squares = jnp.where(lane == 0, high, jnp.where(lane == 1, square - high, 0.0)).astype(bf16)
    pieces, half = out.shape[:2]


    def put(at, value):
        for k in range(pieces):
            out[k, :, at : at + value.shape[1]] = value[k * half : (k + 1) * half]

    put(0, dot(scaled, first[...]).astype(bf16))
    put(2 * own, squares)
    second_copy.wait()
    put(own, dot(scaled, second[...]).astype(bf16))
    shard_copy.wait()


def hidden_terms(arrived, tokens, gain, first, second, shard, peers):
    rows, width = tokens.shape
    return pl.pallas_call(
        hidden_kernel,
        in_specs=[VMEM] * 4 + [ANY] * 2,
        out_specs=(VMEM,) * 3,
        out_shape=(
            pltpu.VMEM((peers, rows // peers, 2 * first.shape[1] + LANES), bf16),
            pltpu.VMEM((rows, width), bf16),
            pltpu.VMEM(shard.shape, shard.dtype),
        ),
        scratch_shapes=[
            pltpu.VMEM(second.shape, second.dtype),
            pltpu.SemaphoreType.DMA((2,)),
        ],
        compiler_params=pltpu.CompilerParams(vmem_limit_bytes=16 << 20),
        name="hidden",
    )(*in_vmem(arrived, tokens, gain, first), second, shard)


def active_kernel(arrived, out):
    count = out.shape[2]
    total = arrived[0].astype(f32)
    for k in range(1, arrived.shape[0]):
        total += arrived[k].astype(f32)
    square = jnp.sum(total[:, count:], axis=1, keepdims=True)
    before = total[:, :count] * lax.rsqrt(square / D + NORM_EPS)
    up = jnp.maximum(before, 0.0)
    low = (up * up).astype(bf16)
    for k in range(out.shape[0]):
        out[k] = low


def active(arrived):
    pieces, rows, width = arrived.shape
    return pl.pallas_call(
        active_kernel,
        in_specs=[VMEM],
        out_specs=VMEM,
        out_shape=pltpu.VMEM((pieces, rows, width - LANES), bf16),
        compiler_params=pltpu.CompilerParams(vmem_limit_bytes=8 << 20),
        name="active",
    )(*in_vmem(arrived))


def shards(
    tokens,
    span_lengths,
    block_state,
    key_cache,
    value_cache,
    decay_cache,
    attn_gain,
    query_weight,
    key_weight,
    value_weight,
    gate_weight,
    decay_matrix,
    decay_offset_bias,
    head_gain,
    out_weight,
    mixer_gain,
    up_weight,
    down_weight,
):
    seq_count, head_count = block_state.shape[:2]
    peers = lax.axis_size("kv")
    core = lax.axis_index("core")
    half = seq_count // CORES
    rows_half = peers * half
    values = head_count * DV

    sent = project(
        tokens, attn_gain, (query_weight, key_weight, decay_matrix, value_weight, gate_weight)
    )
    arrived = exchange(sent.reshape(peers, seq_count, -1), "kv")

    swap = [(c, CORES - 1 - c) for c in range(CORES)]
    out_other = lax.ppermute(out_weight, "core", swap)
    up_other = lax.ppermute(up_weight, "core", swap)
    down_other = lax.ppermute(down_weight, "core", swap)
    out_first = jnp.where(core == 0, out_weight, out_other)
    out_second = jnp.where(core == 0, out_other, out_weight)
    own_tokens = lax.dynamic_index_in_dim(
        tokens.reshape(peers, CORES, half, -1), core, 1, keepdims=False
    ).reshape(rows_half, -1)
    ready = span_terms(
        span_lengths, key_cache, decay_cache, head_gain, decay_offset_bias, mixer_gain
    )
    arrived, out_first, out_second, up_other, down_other, own_tokens, ready = (
        lax.optimization_barrier(
            (arrived, out_first, out_second, up_other, down_other, own_tokens, ready)
        )
    )
    weighted, start_factor, gain, bias, wide_gain = ready

    spread, out_first, out_second = attend(
        arrived,
        weighted,
        start_factor,
        value_cache,
        block_state,
        bias,
        gain,
        (out_first, out_second),
    )
    heads = exchange(spread, ("core", "kv")).reshape(CORES, rows_half, values)
    attn_terms = merge(
        heads[0],
        heads[1],
        out_first,
        out_second,
        lax.axis_size("x"),
    )
    attn_arrived = exchange(attn_terms, "x")
    up_sent, resid, down_other = hidden_terms(
        attn_arrived, own_tokens, wide_gain, up_weight, up_other, down_other, peers
    )
    hidden = active(exchange(up_sent, "kv"))
    every = exchange(hidden, "kv").reshape(rows_half, -1)
    own_count = up_weight.shape[1]
    down_terms = dot(every[:, :own_count], down_weight) + dot(every[:, own_count:], down_other)
    mixer_out = jnp.sum(to_everyone(down_terms.astype(bf16), "x").astype(f32), axis=0)
    own_out = (resid.astype(f32) + mixer_out).astype(bf16)
    other_out = lax.ppermute(own_out, "core", swap)
    low_half = jnp.where(core == 0, own_out, other_out).reshape(peers, half, -1)
    high_half = jnp.where(core == 0, other_out, own_out).reshape(peers, half, -1)
    return jnp.concatenate([low_half, high_half], axis=1).reshape(peers * seq_count, -1)


def solution(mesh):
    sizes = dict(mesh.shape)
    fine = Mesh(
        mesh.devices.reshape(sizes["grp"], sizes["kv"], sizes["tp"] // CORES, CORES),
        ("grp", "kv", "x", "core"),
    )
    tp = ("x", "core")
    placed = (
        P("grp", "kv"),
        P(("grp", "kv")),
        P(("grp", "kv"), tp, None, None),
        P(("grp", "kv"), tp, None),
        P(("grp", "kv"), tp, None),
        P(("grp", "kv"), tp, None),
        P("kv"),
        P("kv", tp),
        P("kv", tp),
        P("kv", tp),
        P("kv", tp),
        P("kv", tp),
        P(tp),
        P(),
        P(tp, "kv"),
        P("kv"),
        P("kv", tp),
        P(tp, "kv"),
    )
    return jax.shard_map(
        shards, mesh=fine, in_specs=placed, out_specs=P("grp", "kv"), check_vma=False
    )
```

```python
import jax
import jax.numpy as jnp
from jax import lax
from jax.experimental import pallas as pl
from jax.experimental.pallas import tpu as pltpu
from jax.sharding import Mesh, PartitionSpec as P

D = 4096
KEY_WIDTH = 32
DV = 64
LANES = 128
SUBLANES = 8
CORES = 2
STAGGER_NS = 4500

NORM_EPS = 1e-06
DECAY_SOFTNESS = 16.0

f32, bf16 = jnp.float32, jnp.bfloat16


def exchange(pieces, axes):
    return lax.all_to_all(pieces, axes, 0, 0, tiled=True)


def to_everyone(value, axes):
    peers = lax.axis_size(axes)
    return exchange(jnp.broadcast_to(value[None], (peers, *value.shape)), axes)


def in_vmem(*values):
    return tuple(pltpu.with_memory_space_constraint(v, pltpu.VMEM) for v in values)


VMEM = pl.BlockSpec(memory_space=pltpu.VMEM)
ANY = pl.BlockSpec(memory_space=pl.ANY)


def dot(a, b):
    return jnp.dot(a, b, preferred_element_type=f32)


def project_kernel(tokens, gain, *refs):
    *weights, out = refs
    rows = tokens[...].astype(f32)
    square = jnp.sum(rows * rows, axis=1, keepdims=True)
    scaled = (rows * gain[...]).astype(bf16)
    start = 0
    for w in weights:
        width = w.shape[1]
        out[:, start : start + width] = dot(scaled, w[...]).astype(bf16)
        start += width
    high = square.astype(bf16).astype(f32)
    lane = lax.broadcasted_iota(jnp.int32, (rows.shape[0], LANES), 1)
    out[:, start:] = jnp.where(lane == 0, high, jnp.where(lane == 1, square - high, 0.0)).astype(
        bf16
    )


def project(tokens, gain, weights):
    width = sum(w.shape[1] for w in weights) + LANES
    return pl.pallas_call(
        project_kernel,
        out_shape=jax.ShapeDtypeStruct((tokens.shape[0], width), bf16),
        name="project",
    )(tokens, gain.reshape(1, -1), *weights)


def span_kernel(
    lengths, keys, decays, head_gain, bias, wide_gain, weighted, start_factor, *small_and_columns
):
    head_gain_out, bias_out, wide_gain_out, columns = small_and_columns
    head_gain_out[...] = jnp.concatenate(
        [head_gain[...]] * (head_gain_out.shape[1] // head_gain.shape[1]), axis=1
    )
    bias_out[...] = bias[...]
    wide_gain_out[...] = wide_gain[...]
    seq_count, channels, span = keys.shape
    place = lax.broadcasted_iota(jnp.int32, (1, span), 1)
    for n in range(seq_count):
        length = lengths[n]
        decay = decays[n]
        last = jnp.sum(jnp.where(place == length - 2, decay, 0.0), axis=1, keepdims=True)
        factor = jnp.where(place < length - 1, jnp.exp(last - decay), 0.0)
        weighted[n] = keys[n].astype(f32) * factor
        columns[:, n : n + 1] = last
    start_factor[...] = jnp.exp(columns[...].T)[:seq_count]


def span_terms(lengths, keys, decays, head_gain, bias, wide_gain):
    seq_count, channels, span = keys.shape
    values = channels // KEY_WIDTH * DV
    return pl.pallas_call(
        span_kernel,
        in_specs=[pl.BlockSpec(memory_space=pltpu.SMEM)] + [VMEM] * 5,
        out_specs=(VMEM,) * 5,
        out_shape=(
            pltpu.VMEM(keys.shape, f32),
            pltpu.VMEM((seq_count, channels), f32),
            pltpu.VMEM((1, values), f32),
            pltpu.VMEM((1, channels), f32),
            pltpu.VMEM((1, wide_gain.shape[0]), f32),
        ),
        scratch_shapes=[pltpu.VMEM((channels, LANES), f32)],
        compiler_params=pltpu.CompilerParams(vmem_limit_bytes=16 << 20),
        name="span",
    )(lengths, keys, decays, *(v.reshape(1, -1) for v in (head_gain, bias, wide_gain)))


def attend_kernel(arrived, weighted, start_factor, bias, gain, values, state, *refs):
    count = len(refs) // 2 - 1
    far, (out, *near, done) = refs[:count], refs[count:]
    copies = [
        pltpu.make_async_copy(a, b, done.at[i]) for i, (a, b) in enumerate(zip(far, near))
    ]
    for copy in copies:
        copy.start()
    seq_count, channels = start_factor.shape
    heads = channels // KEY_WIDTH
    width = heads * DV
    total = arrived[0].astype(f32)
    for k in range(1, arrived.shape[0]):
        total += arrived[k].astype(f32)
    query_sum = total[:, :channels]
    key_sum = total[:, channels : 2 * channels]
    decay_sum = total[:, 2 * channels : 3 * channels]
    value_sum = total[:, 3 * channels : 3 * channels + width]
    gate_sum = total[:, 3 * channels + width : 3 * channels + 2 * width]
    square = jnp.sum(total[:, 3 * channels + 2 * width :], axis=1, keepdims=True)
    scale = lax.rsqrt(square / D + NORM_EPS)
    query = query_sum * scale * KEY_WIDTH ** (-0.5)
    key_new = key_sum * scale
    value_new = value_sum * scale
    gate = gate_sum * scale
    before = decay_sum * scale + bias[...]
    log_sigmoid = jnp.minimum(before, 0.0) - jnp.log1p(jnp.exp(-jnp.abs(before)))
    decayed = query * jnp.exp(log_sigmoid / DECAY_SOFTNESS)

    key_head = lax.broadcasted_iota(jnp.int32, (SUBLANES, channels), 1) // KEY_WIDTH
    key_row = lax.broadcasted_iota(jnp.int32, (SUBLANES, channels), 0)
    value_head = lax.broadcasted_iota(jnp.int32, (SUBLANES, width), 1) // DV
    value_row = lax.broadcasted_iota(jnp.int32, (SUBLANES, width), 0)
    at_start = decayed * start_factor[...]
    padded = jnp.concatenate([decayed, jnp.zeros((LANES - seq_count, channels), f32)], axis=0)
    by_channel = padded.T
    rows = []
    for n in range(seq_count):
        product = weighted[n] * by_channel[:, n : n + 1]
        scores = [
            jnp.sum(product[h * KEY_WIDTH : (h + 1) * KEY_WIDTH], axis=0, keepdims=True)
            for h in range(heads)
        ]
        scores.append(jnp.zeros((SUBLANES - heads, product.shape[1]), f32))
        low = jnp.concatenate(scores, axis=0).astype(bf16)
        history = lax.dot_general(
            low, values[n], (((1,), (1,)), ((), ())), preferred_element_type=f32
        )
        of_heads = jnp.where(key_head == key_row, at_start[n : n + 1], 0.0)
        carried = lax.dot_general(
            of_heads,
            state[n].reshape(channels, DV),
            (((1,), (0,)), ((), ())),
            precision=lax.Precision.HIGHEST,
            preferred_element_type=f32,
        )
        both = history + jnp.concatenate([carried] * heads, axis=1)
        rows.append(jnp.sum(jnp.where(value_head == value_row, both, 0.0), axis=0, keepdims=True))
    raw = jnp.concatenate(rows, axis=0)
    match = query * key_new
    own = jnp.zeros_like(raw)
    column = lax.broadcasted_iota(jnp.int32, raw.shape, 1) // DV
    channel = lax.broadcasted_iota(jnp.int32, match.shape, 1) // KEY_WIDTH
    for h in range(heads):
        amount = jnp.sum(jnp.where(channel == h, match, 0.0), axis=1, keepdims=True)
        own = jnp.where(column == h, amount, own)
    raw = raw + own * value_new
    power = raw * raw
    inverse = jnp.zeros_like(raw)
    for h in range(heads):
        mean = jnp.sum(jnp.where(column == h, power, 0.0), axis=1, keepdims=True) / DV
        inverse = jnp.where(column == h, lax.rsqrt(mean + NORM_EPS), inverse)
    mixed = raw * inverse * gain[...] * (gate * jax.nn.sigmoid(gate))
    half = seq_count // CORES
    low = mixed.astype(bf16)
    for c in range(CORES):
        piece = low[c * half : (c + 1) * half]
        pieces = out.shape[0] // CORES
        for k in range(pieces):
            out[c * pieces + k] = piece
    for copy in copies:
        copy.wait()


def attend(arrived, weighted, start_factor, values, state, bias, gain, shards_far):
    seq_count, width = values.shape[:2]
    half = seq_count // CORES
    count = len(shards_far)
    return pl.pallas_call(
        attend_kernel,
        in_specs=[VMEM] * 7 + [ANY] * count,
        out_specs=(VMEM,) * (1 + count),
        out_shape=(
            pltpu.VMEM((arrived.shape[0] * CORES, half, width), bf16),
            *(pltpu.VMEM(v.shape, v.dtype) for v in shards_far),
        ),
        scratch_shapes=[pltpu.SemaphoreType.DMA((count,))],
        compiler_params=pltpu.CompilerParams(vmem_limit_bytes=16 << 20),
        name="attend",
    )(*in_vmem(arrived, weighted, start_factor, bias, gain, values, state), *shards_far)


def merge_kernel(heads_first, heads_second, first, second, out):
    @pl.when(lax.axis_index("core") == 0)
    def fall_behind():
        pl.delay(STAGGER_NS)

    terms = dot(heads_first[...], first[...]) + dot(heads_second[...], second[...])
    low = terms.astype(bf16)
    for x in range(out.shape[0]):
        out[x] = low


def merge(heads_first, heads_second, first, second, peers):
    shape = (peers, heads_first.shape[0], first.shape[1])
    return pl.pallas_call(
        merge_kernel,
        in_specs=[VMEM] * 4,
        out_specs=VMEM,
        out_shape=pltpu.VMEM(shape, bf16),
        compiler_params=pltpu.CompilerParams(vmem_limit_bytes=8 << 20),
        name="merge",
    )(*in_vmem(heads_first, heads_second, first, second))


def hidden_kernel(
    arrived, tokens, gain, first, second_far, shard_far, out, resid, shard, second, done
):
    second_copy = pltpu.make_async_copy(second_far, second, done.at[0])
    second_copy.start()
    shard_copy = pltpu.make_async_copy(shard_far, shard, done.at[1])
    shard_copy.start()
    total = arrived[0].astype(f32)
    for x in range(1, arrived.shape[0]):
        total += arrived[x].astype(f32)
    low = (tokens[...].astype(f32) + total).astype(bf16)
    resid[...] = low
    rows = low.astype(f32)
    square = jnp.sum(rows * rows, axis=1, keepdims=True)
    scaled = (rows * gain[...]).astype(bf16)
    own = first.shape[1]
    high = square.astype(bf16).astype(f32)
    lane = lax.broadcasted_iota(jnp.int32, (rows.shape[0], LANES), 1)
    squares = jnp.where(lane == 0, high, jnp.where(lane == 1, square - high, 0.0)).astype(bf16)
    pieces, half = out.shape[:2]


    def put(at, value):
        for k in range(pieces):
            out[k, :, at : at + value.shape[1]] = value[k * half : (k + 1) * half]

    put(0, dot(scaled, first[...]).astype(bf16))
    put(2 * own, squares)
    second_copy.wait()
    put(own, dot(scaled, second[...]).astype(bf16))
    shard_copy.wait()


def hidden_terms(arrived, tokens, gain, first, second, shard, peers):
    rows, width = tokens.shape
    return pl.pallas_call(
        hidden_kernel,
        in_specs=[VMEM] * 4 + [ANY] * 2,
        out_specs=(VMEM,) * 3,
        out_shape=(
            pltpu.VMEM((peers, rows // peers, 2 * first.shape[1] + LANES), bf16),
            pltpu.VMEM((rows, width), bf16),
            pltpu.VMEM(shard.shape, shard.dtype),
        ),
        scratch_shapes=[
            pltpu.VMEM(second.shape, second.dtype),
            pltpu.SemaphoreType.DMA((2,)),
        ],
        compiler_params=pltpu.CompilerParams(vmem_limit_bytes=16 << 20),
        name="hidden",
    )(*in_vmem(arrived, tokens, gain, first), second, shard)


def active_kernel(arrived, out):
    count = out.shape[2]
    total = arrived[0].astype(f32)
    for k in range(1, arrived.shape[0]):
        total += arrived[k].astype(f32)
    square = jnp.sum(total[:, count:], axis=1, keepdims=True)
    before = total[:, :count] * lax.rsqrt(square / D + NORM_EPS)
    up = jnp.maximum(before, 0.0)
    low = (up * up).astype(bf16)
    for k in range(out.shape[0]):
        out[k] = low


def active(arrived):
    pieces, rows, width = arrived.shape
    return pl.pallas_call(
        active_kernel,
        in_specs=[VMEM],
        out_specs=VMEM,
        out_shape=pltpu.VMEM((pieces, rows, width - LANES), bf16),
        compiler_params=pltpu.CompilerParams(vmem_limit_bytes=8 << 20),
        name="active",
    )(*in_vmem(arrived))


def shards(
    tokens,
    span_lengths,
    block_state,
    key_cache,
    value_cache,
    decay_cache,
    attn_gain,
    query_weight,
    key_weight,
    value_weight,
    gate_weight,
    decay_matrix,
    decay_offset_bias,
    head_gain,
    out_weight,
    mixer_gain,
    up_weight,
    down_weight,
):
    seq_count, head_count = block_state.shape[:2]
    peers = lax.axis_size("kv")
    core = lax.axis_index("core")
    half = seq_count // CORES
    rows_half = peers * half
    values = head_count * DV

    sent = project(
        tokens, attn_gain, (query_weight, key_weight, decay_matrix, value_weight, gate_weight)
    )
    arrived = exchange(sent.reshape(peers, seq_count, -1), "kv")

    swap = [(c, CORES - 1 - c) for c in range(CORES)]
    out_other = lax.ppermute(out_weight, "core", swap)
    up_other = lax.ppermute(up_weight, "core", swap)
    down_other = lax.ppermute(down_weight, "core", swap)
    out_first = jnp.where(core == 0, out_weight, out_other)
    out_second = jnp.where(core == 0, out_other, out_weight)
    own_tokens = lax.dynamic_index_in_dim(
        tokens.reshape(peers, CORES, half, -1), core, 1, keepdims=False
    ).reshape(rows_half, -1)
    ready = span_terms(
        span_lengths, key_cache, decay_cache, head_gain, decay_offset_bias, mixer_gain
    )
    arrived, out_first, out_second, up_other, down_other, own_tokens, ready = (
        lax.optimization_barrier(
            (arrived, out_first, out_second, up_other, down_other, own_tokens, ready)
        )
    )
    weighted, start_factor, gain, bias, wide_gain = ready

    spread, out_first, out_second = attend(
        arrived,
        weighted,
        start_factor,
        value_cache,
        block_state,
        bias,
        gain,
        (out_first, out_second),
    )
    heads = exchange(spread, ("core", "kv")).reshape(CORES, rows_half, values)
    attn_terms = merge(
        heads[0],
        heads[1],
        out_first,
        out_second,
        lax.axis_size("x"),
    )
    attn_arrived = exchange(attn_terms, "x")
    up_sent, resid, down_other = hidden_terms(
        attn_arrived, own_tokens, wide_gain, up_weight, up_other, down_other, peers
    )
    hidden = active(exchange(up_sent, "kv"))
    every = exchange(hidden, "kv").reshape(rows_half, -1)
    own_count = up_weight.shape[1]
    down_terms = dot(every[:, :own_count], down_weight) + dot(every[:, own_count:], down_other)
    mixer_out = jnp.sum(to_everyone(down_terms.astype(bf16), "x").astype(f32), axis=0)
    own_out = (resid.astype(f32) + mixer_out).astype(bf16)
    other_out = lax.ppermute(own_out, "core", swap)
    low_half = jnp.where(core == 0, own_out, other_out).reshape(peers, half, -1)
    high_half = jnp.where(core == 0, other_out, own_out).reshape(peers, half, -1)
    return jnp.concatenate([low_half, high_half], axis=1).reshape(peers * seq_count, -1)


def solution(mesh):
    sizes = dict(mesh.shape)
    fine = Mesh(
        mesh.devices.reshape(sizes["grp"], sizes["kv"], sizes["tp"] // CORES, CORES),
        ("grp", "kv", "x", "core"),
    )
    tp = ("x", "core")
    placed = (
        P("grp", "kv"),
        P(("grp", "kv")),
        P(("grp", "kv"), tp, None, None),
        P(("grp", "kv"), tp, None),
        P(("grp", "kv"), tp, None),
        P(("grp", "kv"), tp, None),
        P("kv"),
        P("kv", tp),
        P("kv", tp),
        P("kv", tp),
        P("kv", tp),
        P("kv", tp),
        P(tp),
        P(),
        P(tp, "kv"),
        P("kv"),
        P("kv", tp),
        P(tp, "kv"),
    )
    return jax.shard_map(
        shards, mesh=fine, in_specs=placed, out_specs=P("grp", "kv"), check_vma=False
    )
```
